128 devices in a mesh: ep: 16 (over z, x), tp: 8 (over y, core).
Axes of the slice: x: 4, y: 4, z: 4, core: 2. Of those that a mesh axis runs over, the one named last changes fastest.
Arguments:
- tokens: bfloat16 [512, 2048], P('ep'), may hold values from -6 to 6
- state: float32 [512, 16, 128, 128], P('ep', 'tp'), may hold values from -6 to 6
- norm_gain: float32 [2048], replicated, may hold values from 0.1 to 1.9
- w_query: bfloat16 [2048, 2048], P(None, 'tp'), may hold values from -0.125 to 0.125
- w_forget: bfloat16 [2048, 2048], P(None, 'tp'), may hold values from -0.125 to 0.125
- w_input: bfloat16 [2048, 2048], P(None, 'tp'), may hold values from -0.125 to 0.125
- w_outgate: bfloat16 [2048, 2048], P(None, 'tp'), may hold values from -0.125 to 0.125
- forget_floor: float32 [2048], P('tp'), may hold values from 0.05 to 0.95
- head_gain: float32 [128], replicated, may hold values from 0.1 to 1.9
- w_out: bfloat16 [2048, 2048], P('tp'), may hold values from -0.125 to 0.125
- ffn_gain: float32 [2048], replicated, may hold values from 0.1 to 1.9
- routes: int32 [512, 2], P('ep'), may hold values from 0 to 15, all different within a row; in each aligned block of 32 rows (0 to 31, 32 to 63, ...) at most 8 rows name the same one
- route_weights: float32 [512, 2], P('ep'), may hold values from 0.2 to 1
- expert_gate: bfloat16 [16, 2048, 5632], P('ep', None, 'tp'), may hold values from -0.125 to 0.125
- expert_up: bfloat16 [16, 2048, 5632], P('ep', None, 'tp'), may hold values from -0.125 to 0.125
- expert_down: bfloat16 [16, 5632, 2048], P('ep', 'tp'), may hold values from -0.078125 to 0.078125
- dense_gate: bfloat16 [2048, 5632], P(None, 'ep'), may hold values from -0.125 to 0.125
- dense_up: bfloat16 [2048, 5632], P(None, 'ep'), may hold values from -0.125 to 0.125
- dense_down: bfloat16 [5632, 2048], P('ep'), may hold values from -0.078125 to 0.078125
- dense_mix: float32 [2048], replicated, may hold values from -6 to 6
Outputs:
- mixed: bfloat16 [512, 2048], P('ep')
- new_state: float32 [512, 16, 128, 128], P('ep', 'tp')
The draws below stay inside these ranges and needn't reach their ends.
Inputs may be any that keep to these rules, and one draw needn't show every extreme that they name: `routes`: each row names 2 different experts; the rows of one index of ep name no expert more than 8 times, a bound that some block reaches.
All inputs are finite; a program needn't handle non-finite values.
Results may differ from the reference program's by a relative error of at most 0.014.
Values may be sent and summed in bfloat16 or wider, within the bound.
No kernel may reach another device: no remote copies, remote signals or barrier semaphores. Data moves between devices by JAX's collectives and lax.ppermute only.
A program may use at most 128 MiB of HBM per device.

```python
import math
import jax
import jax.numpy as jnp
import numpy as np
from jax import lax

D = 2048
HEADS = 16
DK = 128
DV = 128
EFF = 5632
DFF = 5632
TOP = 2
SEQ_DEV = 32
EXPERTS = 16
CAP = 8
TOKENS = 512
N_EP = 16
N_TP = 8


def levels(own_key, extent, pieces, least, top_value):
    def one(axis_at, blocks):
        steps = jax.random.uniform(jax.random.fold_in(jax.random.fold_in(own_key, 6), axis_at), (blocks,), jnp.float32, least / len(pieces), top_value / len(pieces))
        return jnp.repeat(jnp.exp(steps), extent[axis_at] // blocks).reshape((-1,) + (1,) * (len(extent) - axis_at - 1))

    factor_of = one(*pieces[0])
    for cut in pieces[1:]:
        factor_of = factor_of * one(*cut)
    return factor_of


def routed_block(key, own, number, rows, amount, top, limit, lean):
    order = jax.random.permutation(key, amount)
    packed, usual = load_shares(amount, rows * top, limit, lean, True), load_shares(amount, rows * top, limit, lean, False)
    places = jnp.arange(amount)

    def named(sizes, offset_by):
        used = int((sizes > 0).sum())
        fixed = max(1, used // 4)
        moved = fixed + (places - fixed + offset_by * (used - fixed)) % max(1, amount - fixed)
        return jnp.zeros((amount,), jnp.int32).at[order[jnp.where(places < fixed, places, moved)]].set(jnp.asarray(sizes, jnp.int32))

    sizes = jnp.where(number % 4 == 0, named(packed, number // 4), named(usual, number - number // 4 - 1))
    mixed = jax.random.permutation(jax.random.fold_in(own, 3), amount)
    donor, receiver = mixed[0:amount // 2 * 2:2], mixed[1:amount // 2 * 2:2]
    slack = jnp.minimum(sizes[donor] - 1, limit - sizes[receiver]) // 2
    slack = jnp.where((donor == order[0]) | (receiver == order[0]) | (sizes[receiver] == 0), 0, jnp.maximum(slack, 0))
    moved = jax.random.randint(jax.random.fold_in(own, 4), (amount // 2,), 0, 1 << 20) % (slack + 1)
    sizes = sizes.at[donor].add(-moved).at[receiver].add(moved)
    items = jnp.searchsorted(jnp.cumsum(sizes), jnp.arange(rows * top), side="right").astype(jnp.int32)
    listing = items.reshape(top, rows).T
    listing = listing[jax.random.permutation(jax.random.fold_in(own, 1), rows)]
    offset_by = jax.random.randint(jax.random.fold_in(own, 2), (rows, 1), 0, top)
    return jnp.take_along_axis(listing, (jnp.arange(top)[None, :] + offset_by) % top, axis=1)


def load_shares(amount, total, reach, slope, full):
    weights = [(1 << 20) // math.isqrt(rank ** slope) + 1 for rank in range(1, amount + 1)]
    largest = reach if full else min(reach, max(-(-total // amount), total * weights[0] // sum(weights)))
    least = 1 if total - largest >= amount - 1 else 0
    holding, spare = [largest] + [least] * (amount - 1), total - largest - least * (amount - 1)
    while spare > 0:
        movable = [i for i in range(1, amount) if holding[i] < largest] or [i for i in range(1, amount) if holding[i] < reach]
        whole, budget = sum([weights[i] for i in movable]), spare
        for i in movable:
            extra = min(reach - holding[i], max(1, budget * weights[i] // whole), spare)
            holding[i] = holding[i] + extra
            spare = spare - extra
    return np.array(holding)


def gaussian(rng, shape, width, reach, shards=(), kind=jnp.bfloat16):
    array = width * jax.random.normal(rng, shape, jnp.float32)
    if shards:
        array = array * levels(rng, shape, shards, -0.22, 0.18)
    return jnp.clip(array, -reach, reach).astype(kind)


def setup_inputs(seed: int = 0) -> dict:
    key_list = jax.random.split(jax.random.key(seed), 21)
    tokens = gaussian(key_list[0], (TOKENS, D), 1.0, 6.0, ((0, 16),))
    state = gaussian(key_list[1], (TOKENS, HEADS, DK, DV), 1.0, 6.0, ((0, 16), (1, 8)), jnp.float32)
    norm_gain = jnp.clip(1.0 + 0.18 * jax.random.normal(key_list[2], (D,), jnp.float32), 0.1, 1.9)
    w_query = gaussian(key_list[3], (D, HEADS * DK), D ** -0.5, 0.125, ((1, 8),))
    w_forget = gaussian(key_list[4], (D, HEADS * DK), D ** -0.5, 0.125, ((1, 8),))
    w_input = gaussian(key_list[5], (D, HEADS * DV), D ** -0.5, 0.125, ((1, 8),))
    w_outgate = gaussian(key_list[6], (D, HEADS * DV), D ** -0.5, 0.125, ((1, 8),))
    forget_floor = jnp.clip(0.05 + 0.9 * jax.random.uniform(key_list[7], (HEADS * DK,), jnp.float32) ** levels(key_list[7], (HEADS * DK,), ((0, 8),), -0.2, 0.2), 0.05, 0.95)
    head_gain = jnp.clip(1.0 + 0.18 * jax.random.normal(key_list[8], (DV,), jnp.float32), 0.1, 1.9)
    w_out = gaussian(key_list[9], (HEADS * DV, D), (HEADS * DV) ** -0.5, 0.125, ((0, 8),))
    ffn_gain = jnp.clip(1.0 + 0.18 * jax.random.normal(key_list[10], (D,), jnp.float32), 0.1, 1.9)
    routes_keys = jax.random.split(jax.random.fold_in(key_list[11], 1), TOKENS // SEQ_DEV)
    routes_turns = jax.random.permutation(jax.random.fold_in(key_list[11], 3), TOKENS // SEQ_DEV)
    routes = jax.vmap(lambda own, number: routed_block(jax.random.fold_in(key_list[11], 2), own, number, SEQ_DEV, EXPERTS, TOP, CAP, 2))(routes_keys, routes_turns).reshape((TOKENS, TOP))
    route_weights = jnp.clip(0.2 + 0.8 * jax.random.uniform(key_list[12], (TOKENS, TOP), jnp.float32) ** levels(key_list[12], (TOKENS, TOP), ((0, 16),), -0.2, 0.2), 0.2, 1.0)
    expert_gate = gaussian(key_list[13], (EXPERTS, D, EFF), D ** -0.5, 0.125, ((0, 16), (2, 8)))
    expert_up = gaussian(key_list[14], (EXPERTS, D, EFF), D ** -0.5, 0.125, ((0, 16), (2, 8)))
    expert_down = gaussian(key_list[15], (EXPERTS, EFF, D), EFF ** -0.5, 0.078125, ((0, 16), (1, 8)))
    dense_gate = gaussian(key_list[16], (D, DFF), D ** -0.5, 0.125, ((1, 16),))
    dense_up = gaussian(key_list[17], (D, DFF), D ** -0.5, 0.125, ((1, 16),))
    dense_down = gaussian(key_list[18], (DFF, D), DFF ** -0.5, 0.078125, ((0, 16),))
    dense_mix = gaussian(key_list[19], (D,), 1.5, 6.0, (), jnp.float32)
    return dict(tokens=tokens, state=state, norm_gain=norm_gain, w_query=w_query, w_forget=w_forget, w_input=w_input, w_outgate=w_outgate, forget_floor=forget_floor, head_gain=head_gain, w_out=w_out, ffn_gain=ffn_gain, routes=routes, route_weights=route_weights, expert_gate=expert_gate, expert_up=expert_up, expert_down=expert_down, dense_gate=dense_gate, dense_up=dense_up, dense_down=dense_down, dense_mix=dense_mix)


EPS = 1e-06

def rounded(value):
    return lax.optimization_barrier(value.astype(jnp.bfloat16)).astype(jnp.float32)

def rms_norm(value, gain):
    return value * lax.rsqrt(lax.optimization_barrier(jnp.mean(value * value, axis=-1, keepdims=True)) + EPS) * gain

def make_table(group_routes, experts, capacity):
    flat = group_routes.reshape(-1)
    onehot = (flat[:, None] == jnp.arange(experts, dtype=jnp.int32)[None, :]).astype(jnp.int32)
    before = jnp.cumsum(onehot, axis=0) - onehot
    slot = lax.optimization_barrier(jnp.sum(before * onehot, axis=1))
    where = flat * capacity + slot
    return (where[:, None] == jnp.arange(experts * capacity, dtype=jnp.int32)[None, :]).astype(jnp.float32)

def reference(tokens, state, norm_gain, w_query, w_forget, w_input, w_outgate, forget_floor, head_gain, w_out, ffn_gain, routes, route_weights, expert_gate, expert_up, expert_down, dense_gate, dense_up, dense_down, dense_mix):
    resid_in = tokens.astype(jnp.float32)
    normed = rms_norm(resid_in, norm_gain).astype(jnp.bfloat16)
    zq = jnp.dot(normed, w_query, preferred_element_type=jnp.float32)
    zf = jnp.dot(normed, w_forget, preferred_element_type=jnp.float32)
    zi = jnp.dot(normed, w_input, preferred_element_type=jnp.float32)
    zg = jnp.dot(normed, w_outgate, preferred_element_type=jnp.float32)
    logf = jnp.logaddexp(jax.nn.log_sigmoid(zf), jnp.log(forget_floor) + jax.nn.log_sigmoid(-zf))
    logf = logf.reshape(TOKENS, HEADS, DK)
    query = jax.nn.silu(zq).reshape(TOKENS, HEADS, DK)
    keep = jnp.exp(logf)
    write = -jnp.expm1(logf)
    values = zi.reshape(TOKENS, HEADS, DV)
    new_state = keep[..., None] * state + write[..., None] * values[:, :, None, :]
    read = jnp.einsum('thk,thkv->thv', query, new_state, precision=lax.Precision.HIGHEST)
    read = rms_norm(read, head_gain).reshape(TOKENS, HEADS * DV)
    headout = (read * jax.nn.silu(zg)).astype(jnp.bfloat16)
    blocks = jnp.einsum('tnc,ncd->ntd', headout.reshape(TOKENS, N_TP, -1).astype(jnp.float32), w_out.reshape(N_TP, -1, D).astype(jnp.float32))
    mixout = lax.optimization_barrier(jnp.sum(rounded(blocks), axis=0))
    resid = resid_in + mixout
    ffn_in = rms_norm(resid, ffn_gain).astype(jnp.bfloat16)
    group_routes = routes.reshape(N_EP, SEQ_DEV, TOP)
    tables = jax.vmap(lambda r: make_table(r, EXPERTS, CAP))(group_routes)
    repeated = jnp.repeat(ffn_in.reshape(N_EP, SEQ_DEV, D), TOP, axis=1).astype(jnp.float32)
    sent = jnp.einsum('grp,grd->gpd', tables, repeated).astype(jnp.bfloat16)
    arrived = sent.reshape(N_EP, EXPERTS, CAP, D).transpose(1, 0, 2, 3).reshape(EXPERTS, N_EP * CAP, D)

    def one_expert(items):
        rows, gate_w, up_w, down_w = items
        gate = jnp.dot(rows, gate_w, preferred_element_type=jnp.float32)
        upper = jnp.dot(rows, up_w, preferred_element_type=jnp.float32)
        hidden = (jax.nn.silu(gate) * upper).astype(jnp.bfloat16)
        parts = jnp.einsum('rnc,ncd->nrd', hidden.reshape(rows.shape[0], N_TP, -1).astype(jnp.float32), down_w.reshape(N_TP, -1, D).astype(jnp.float32))
        return lax.optimization_barrier(jnp.sum(rounded(parts), axis=0)).astype(jnp.bfloat16)
    outputs = lax.map(one_expert, (arrived, expert_gate, expert_up, expert_down))
    back = outputs.reshape(EXPERTS, N_EP, CAP, D).transpose(1, 0, 2, 3).reshape(N_EP, EXPERTS * CAP, D)
    picked = jnp.einsum('grp,gpd->grd', tables, back.astype(jnp.float32))
    weighted = picked * route_weights.reshape(N_EP, SEQ_DEV * TOP)[:, :, None]
    moe = lax.optimization_barrier(jnp.sum(weighted.reshape(N_EP, SEQ_DEV, TOP, D), axis=2)).reshape(TOKENS, D)
    dgate = jnp.dot(ffn_in, dense_gate, preferred_element_type=jnp.float32)
    dupper = jnp.dot(ffn_in, dense_up, preferred_element_type=jnp.float32)
    dense_hidden = (jax.nn.silu(dgate) * dupper).astype(jnp.bfloat16)
    dense = rounded(jnp.dot(dense_hidden, dense_down, preferred_element_type=jnp.float32))
    mixed = (resid + moe + jax.nn.sigmoid(dense_mix) * dense).astype(jnp.bfloat16)
    return (mixed, new_state)
```

```python
import jax
import jax.numpy as jnp
from jax import lax
from jax.sharding import PartitionSpec as P

EPS = 1e-06
F32 = jnp.float32
BF16 = jnp.bfloat16


def rms_norm(value, gain):
    return value * lax.rsqrt(jnp.mean(value * value, axis=-1, keepdims=True) + EPS) * gain


def routing(local_routes, experts, capacity):
    flat = local_routes.reshape(-1)
    onehot = (flat[:, None] == jnp.arange(experts, dtype=jnp.int32)[None, :]).astype(jnp.int32)
    before = jnp.cumsum(onehot, axis=0) - onehot
    slot = jnp.sum(before * onehot, axis=1)
    where = (flat * capacity + slot).reshape(local_routes.shape)
    return where[:, :, None] == jnp.arange(experts * capacity, dtype=jnp.int32)[None, None, :]


def core_swap(x):
    return lax.ppermute(x, "tp", [(t, t ^ 1) for t in range(8)])


def row_sum(x):
    mine = x.astype(BF16)
    other = lax.ppermute(mine, "tp", [(t, t ^ 2) for t in range(8)])
    mine = (mine.astype(F32) + other.astype(F32)).astype(BF16)
    other = lax.ppermute(mine, "tp", [(t, (6 - t // 2 * 2) + t % 2) for t in range(8)])
    return mine.astype(F32) + other.astype(F32)


def half_sum(x, core):
    rows = x.shape[0] // 2
    mine = lax.dynamic_slice_in_dim(x, core * rows, rows, 0)
    theirs = lax.dynamic_slice_in_dim(x, (1 - core) * rows, rows, 0)
    mine = mine.astype(BF16).astype(F32) + core_swap(theirs.astype(BF16)).astype(F32)
    return row_sum(mine)


def both_halves(mine, core):
    other = core_swap(mine)
    first = jnp.where(core == 0, mine, other)
    second = jnp.where(core == 0, other, mine)
    return jnp.concatenate([first, second], axis=0)


def local(
    tokens,
    state,
    norm_gain,
    w_query,
    w_forget,
    w_input,
    w_outgate,
    forget_floor,
    head_gain,
    w_out,
    ffn_gain,
    routes,
    route_weights,
    expert_gate,
    expert_up,
    expert_down,
    dense_gate,
    dense_up,
    dense_down,
    dense_mix,
):
    seqs, width = tokens.shape
    heads, key_size, value_size = state.shape[1:]
    tp = lax.axis_index("tp")
    core = tp % 2
    half = seqs // 2
    normed = rms_norm(tokens.astype(F32), norm_gain).astype(BF16)
    zq = jnp.dot(normed, w_query, preferred_element_type=F32)
    zf = jnp.dot(normed, w_forget, preferred_element_type=F32)
    zi = jnp.dot(normed, w_input, preferred_element_type=F32)
    zg = jnp.dot(normed, w_outgate, preferred_element_type=F32)
    keep = forget_floor + (1 - forget_floor) * jax.nn.sigmoid(zf)
    write = (1 - forget_floor) * jax.nn.sigmoid(-zf)
    keep = keep.reshape(seqs, heads, key_size)
    write = write.reshape(seqs, heads, key_size)
    query = jax.nn.silu(zq).reshape(seqs, heads, key_size)
    values = zi.reshape(seqs, heads, value_size)
    new_state = keep[..., None] * state + write[..., None] * values[:, :, None, :]
    read = jnp.sum(query[..., None] * new_state, axis=2)
    read = rms_norm(read, head_gain).reshape(seqs, heads * value_size)
    headout = (read * jax.nn.silu(zg)).astype(BF16)
    block_term = jnp.dot(headout, w_out, preferred_element_type=F32)

    mixout = half_sum(block_term, core)
    resid = lax.dynamic_slice_in_dim(tokens, core * half, half, 0).astype(F32) + mixout
    ffn_half = rms_norm(resid, ffn_gain).astype(BF16)
    ffn_in = both_halves(ffn_half, core)

    groups = lax.axis_size("ep")
    experts = groups * expert_gate.shape[0]
    top = routes.shape[1]
    capacity = 2 * seqs * top // experts
    share_rows = seqs // lax.axis_size("tp")
    wide = share_rows * width // capacity
    hits = routing(routes, experts, capacity)
    table = jnp.any(hits, axis=1).astype(BF16)
    sent = jnp.dot(table.T, ffn_in, preferred_element_type=F32).astype(BF16)
    sent = sent.reshape(experts, capacity, width)
    mine = lax.dynamic_slice_in_dim(ffn_in, tp * share_rows, share_rows, 0)
    mine = jnp.broadcast_to(mine.reshape(1, capacity, wide), (groups, capacity, wide))
    packet = jnp.concatenate([sent, mine], axis=2)
    packet = lax.all_to_all(packet, "ep", split_axis=0, concat_axis=0, tiled=True)
    rows = packet[:, :, :width].reshape(groups * capacity, width)
    piece = packet[:, :, width:].reshape(groups * share_rows, width)

    gate = jnp.dot(rows, expert_gate[0], preferred_element_type=F32)
    upper = jnp.dot(rows, expert_up[0], preferred_element_type=F32)
    hidden = (jax.nn.silu(gate) * upper).astype(BF16)
    part = jnp.dot(hidden, expert_down[0], preferred_element_type=F32).astype(BF16)
    dgate = jnp.dot(piece, dense_gate, preferred_element_type=F32)
    dupper = jnp.dot(piece, dense_up, preferred_element_type=F32)
    dhidden = (jax.nn.silu(dgate) * dupper).astype(BF16)
    dpart = jnp.dot(dhidden, dense_down, preferred_element_type=F32).astype(BF16)
    packet = jnp.concatenate(
        [part.reshape(groups, capacity, width), dpart.reshape(groups, capacity, wide)], axis=2
    )
    packet = lax.all_to_all(packet, "ep", split_axis=0, concat_axis=0, tiled=True)
    back = packet[:, :, :width].reshape(experts * capacity, width)
    dense = packet[:, :, width:].astype(F32).sum(axis=0).reshape(share_rows, width)

    pick = jnp.sum(hits * route_weights[:, :, None], axis=1)
    high = pick.astype(BF16)
    low = (pick - high.astype(F32)).astype(BF16)
    moe = jnp.dot(jnp.concatenate([high, low]), back, preferred_element_type=F32)
    moe = moe[:seqs] + moe[seqs:]
    dense = jax.nn.sigmoid(dense_mix) * dense
    at = jnp.arange(seqs, dtype=jnp.int32)[:, None] - tp * share_rows
    for r in range(share_rows):
        moe = moe + jnp.where(at == r, dense[r][None], 0.0)
    added = half_sum(moe, core)
    mixed = both_halves((resid + added).astype(BF16), core)
    return (mixed, new_state)


def solution(mesh):
    in_specs = (
        P("ep", None),
        P("ep", "tp", None, None),
        P(),
        P(None, "tp"),
        P(None, "tp"),
        P(None, "tp"),
        P(None, "tp"),
        P("tp"),
        P(),
        P("tp", None),
        P(),
        P("ep", None),
        P("ep", None),
        P("ep", None, "tp"),
        P("ep", None, "tp"),
        P("ep", "tp", None),
        P(None, "ep"),
        P(None, "ep"),
        P("ep", None),
        P(),
    )
    out_specs = (P("ep", None), P("ep", "tp", None, None))
    return jax.shard_map(local, mesh=mesh, in_specs=in_specs, out_specs=out_specs, check_vma=False)
```

```python
import jax
import jax.numpy as jnp
from jax import lax
from jax.experimental import pallas as pl
from jax.experimental.pallas import tpu as pltpu
from jax.sharding import PartitionSpec as P

EPS = 1e-06
F32 = jnp.float32
BF16 = jnp.bfloat16
ANY = pl.BlockSpec(memory_space=pl.ANY)
VMEM = pl.BlockSpec(memory_space=pltpu.VMEM)


CHUNKS = 4


def dot(a, b):
    return jnp.dot(a, b, preferred_element_type=F32)


def mean_scale(x):
    return lax.rsqrt(jnp.mean(x * x, axis=-1, keepdims=True) + EPS)


def sigmoid(x):
    return 1.0 / (1.0 + jnp.exp(-x))


def mixer_kernel(
    tokens,
    gain,
    floor,
    head_gain,
    state,
    w_query,
    w_forget,
    w_input,
    w_outgate,
    w_out,
    new_state,
    mine,
    theirs,
    w_buf,
    wo_buf,
    held,
    keep_t,
    query_t,
    values,
    read,
    w_sem,
    wo_sem,
    in_sem,
    out_sem,
):
    seqs = tokens.shape[0]
    heads, size = held.shape[1:3]
    step = seqs // CHUNKS
    core = lax.rem(lax.axis_index("tp"), 2)
    loads = [
        pltpu.make_async_copy(w, w_buf.at[i], w_sem.at[i])
        for i, w in enumerate((w_forget, w_query, w_input, w_outgate))
    ]
    for load in loads[:3]:
        load.start()

    def fetch(j):
        rows = pl.ds(j * step, step)
        return pltpu.make_async_copy(state.at[rows], held.at[rows], in_sem.at[j])

    def flush(j):
        rows = pl.ds(j * step, step)
        return pltpu.make_async_copy(held.at[rows], new_state.at[rows], out_sem.at[j])

    for j in range(CHUNKS):
        fetch(j).start()
    loads[3].start()
    load_out = pltpu.make_async_copy(w_out, wo_buf, wo_sem)
    load_out.start()

    x = tokens[...].astype(F32)
    normed = (x * mean_scale(x) * gain[...]).astype(BF16)
    base = floor[...]
    loads[0].wait()
    keep = (base + (1.0 - base) * sigmoid(dot(normed, w_buf[0]))).T
    loads[1].wait()
    zq = dot(normed, w_buf[1])
    query = (zq * sigmoid(zq)).T
    for j in range(CHUNKS):
        keep_t[j, :, :] = keep[:, j * step : (j + 1) * step]
        query_t[j, :, :] = query[:, j * step : (j + 1) * step]
    loads[2].wait()
    values[...] = dot(normed, w_buf[2])

    def body(j, carry):
        fetch(j).wait()
        rows = pl.ds(pl.multiple_of(j * step, step), step)
        block = values[rows, :]
        reads = []
        for i in range(step):
            parts = []
            for h in range(heads):
                lanes = slice(h * size, (h + 1) * size)
                v = block[i : i + 1, lanes]
                k = jnp.broadcast_to(keep_t[j, lanes, i : i + 1], (size, size))
                q = jnp.broadcast_to(query_t[j, lanes, i : i + 1], (size, size))
                new = v + k * (held[j * step + i, h] - v)
                held[j * step + i, h] = new
                parts.append(jnp.sum(q * new, axis=0, keepdims=True))
            reads.append(jnp.concatenate(parts, axis=1))
        read[rows, :] = jnp.concatenate(reads, axis=0)
        flush(j).start()
        return carry

    lax.fori_loop(0, CHUNKS, body, 0)
    loads[3].wait()
    zg = dot(normed, w_buf[3])
    gate = zg * sigmoid(zg)
    outs = []
    for h in range(heads):
        lanes = slice(h * size, (h + 1) * size)
        r = read[:, lanes]
        outs.append(r * mean_scale(r) * head_gain[...] * gate[:, lanes])
    headout = jnp.concatenate(outs, axis=1).astype(BF16)
    load_out.wait()
    block = dot(headout, wo_buf[...])
    half = seqs // 2
    first = core == 0
    mine[...] = jnp.where(first, block[:half], block[half:]).astype(BF16)
    theirs[...] = jnp.where(first, block[half:], block[:half]).astype(BF16)
    for j in range(CHUNKS):
        flush(j).wait()


def mixer(tokens, state, norm_gain, w_query, w_forget, w_input, w_outgate, floor, head_gain, w_out):
    seqs, width = tokens.shape
    channels = w_query.shape[1]
    half = jax.ShapeDtypeStruct((seqs // 2, width), BF16)
    step = seqs // CHUNKS
    return pl.pallas_call(
        mixer_kernel,
        out_shape=(jax.ShapeDtypeStruct(state.shape, state.dtype), half, half),
        in_specs=[VMEM] * 4 + [ANY] * 6,
        out_specs=(ANY, VMEM, VMEM),
        scratch_shapes=[
            pltpu.VMEM((4, width, channels), BF16),
            pltpu.VMEM((channels, width), BF16),
            pltpu.VMEM(state.shape, F32),
            pltpu.VMEM((CHUNKS, channels, step), F32),
            pltpu.VMEM((CHUNKS, channels, step), F32),
            pltpu.VMEM((seqs, channels), F32),
            pltpu.VMEM((seqs, channels), F32),
            pltpu.SemaphoreType.DMA((4,)),
            pltpu.SemaphoreType.DMA,
            pltpu.SemaphoreType.DMA((CHUNKS,)),
            pltpu.SemaphoreType.DMA((CHUNKS,)),
        ],
        compiler_params=pltpu.CompilerParams(vmem_limit_bytes=20 << 20),
        name="mixer",
    )(
        tokens,
        norm_gain.reshape(1, width),
        floor.reshape(1, channels),
        head_gain.reshape(1, -1),
        state,
        w_query,
        w_forget,
        w_input,
        w_outgate,
        w_out,
    )


def build_kernel(table, share, mine, other, packet):
    width = mine.shape[1]
    wide = packet.shape[1] - width
    rows = jnp.concatenate([mine[...], other[...]], axis=0)
    packet[:, :width] = dot(table[...], rows).astype(BF16)
    part = dot(share[...], rows)
    half = part.shape[0] // 2
    part = jnp.concatenate([part[:half, :wide], part[half:, wide:]], axis=0)
    copies = packet.shape[0] // part.shape[0]
    packet[:, width:] = jnp.concatenate([part] * copies, axis=0).astype(BF16)


def build(table, share, mine, other, wide):
    slots, width = table.shape[0], mine.shape[1]
    return pl.pallas_call(
        build_kernel,
        out_shape=jax.ShapeDtypeStruct((slots, width + wide), BF16),
        in_specs=[VMEM] * 4,
        out_specs=VMEM,
        compiler_params=pltpu.CompilerParams(vmem_limit_bytes=8 << 20),
        name="build",
    )(table, share, mine, other)


def in_group_turn(x, group):
    rows, lanes = x.shape
    x = x.reshape(rows // group, group, lanes)
    return pltpu.roll(x, group // 2, axis=1).reshape(rows, lanes)


def ffn_kernel(packet, e_gate, e_up, e_down, d_gate, d_up, d_down, out):
    width = e_gate.shape[0]
    wide = packet.shape[1] - width
    group = 8
    rows = packet[:, :width]
    gate = dot(rows, e_gate[...])
    upper = dot(rows, e_up[...])
    hidden = (gate * sigmoid(gate) * upper).astype(BF16)
    out[:, :width] = dot(hidden, e_down[...]).astype(BF16)
    share = packet[:, width:]
    gate = dot(share, d_gate[:wide, :]) + in_group_turn(dot(share, d_gate[wide:, :]), group)
    upper = dot(share, d_up[:wide, :]) + in_group_turn(dot(share, d_up[wide:, :]), group)
    hidden = (gate * sigmoid(gate) * upper).astype(BF16)
    result = dot(hidden, d_down[...])
    turned = in_group_turn(result[:, wide:], group)
    at = lax.broadcasted_iota(jnp.int32, turned.shape, 0)
    out[:, width:] = jnp.where(at % group < group // 2, result[:, :wide], turned).astype(BF16)


def ffn(packet, e_gate, e_up, e_down, d_gate, d_up, d_down):
    return pl.pallas_call(
        ffn_kernel,
        out_shape=jax.ShapeDtypeStruct(packet.shape, BF16),
        in_specs=[VMEM] * 7,
        out_specs=VMEM,
        compiler_params=pltpu.CompilerParams(vmem_limit_bytes=32 << 20),
        name="ffn",
    )(packet, e_gate, e_up, e_down, d_gate, d_up, d_down)


def combine_kernel(pick, packet, mix, place, mine, theirs):
    width = mix.shape[1]
    wide = packet.shape[1] - width
    half = mine.shape[0]
    group = 8
    moe = dot(pick[...], packet[:, :width])
    moe = moe[: 2 * half] + moe[2 * half :]
    parts = packet[:, width:].astype(F32)
    parts = jnp.sum(parts.reshape(-1, group, wide), axis=0)
    dense = jnp.concatenate([parts[: group // 2], parts[group // 2 :]], axis=1)
    dense = sigmoid(mix[...]) * dense
    total = moe[:half]
    where = place[...]
    for r in range(group // 2):
        total = total + where[:, r : r + 1] * dense[r : r + 1]
    mine[...] = total.astype(BF16)
    theirs[...] = moe[half:].astype(BF16)


def combine(pick, packet, mix, place):
    width = mix.shape[0]
    half = jax.ShapeDtypeStruct((pick.shape[0] // 4, width), BF16)
    return pl.pallas_call(
        combine_kernel,
        out_shape=(half, half),
        in_specs=[VMEM] * 4,
        out_specs=(VMEM, VMEM),
        compiler_params=pltpu.CompilerParams(vmem_limit_bytes=8 << 20),
        name="combine",
    )(pick, packet, mix.reshape(1, width), place)


def routing(local_routes, experts, capacity):
    flat = local_routes.reshape(-1)
    onehot = (flat[:, None] == jnp.arange(experts, dtype=jnp.int32)[None, :]).astype(jnp.int32)
    before = jnp.cumsum(onehot, axis=0) - onehot
    slot = jnp.sum(before * onehot, axis=1)
    where = (flat * capacity + slot).reshape(local_routes.shape)
    return where[:, :, None] == jnp.arange(experts * capacity, dtype=jnp.int32)[None, None, :]


def core_swap(x):
    return lax.ppermute(x, "tp", [(t, t ^ 1) for t in range(8)])


def row_sum(mine, theirs):
    other = core_swap(theirs)
    mine = (mine.astype(F32) + other.astype(F32)).astype(BF16)
    other = lax.ppermute(mine, "tp", [(t, t ^ 2) for t in range(8)])
    mine = (mine.astype(F32) + other.astype(F32)).astype(BF16)
    other = lax.ppermute(mine, "tp", [(t, (6 - t // 2 * 2) + t % 2) for t in range(8)])
    return mine.astype(F32) + other.astype(F32)


def local(
    tokens,
    state,
    norm_gain,
    w_query,
    w_forget,
    w_input,
    w_outgate,
    forget_floor,
    head_gain,
    w_out,
    ffn_gain,
    routes,
    route_weights,
    expert_gate,
    expert_up,
    expert_down,
    dense_gate,
    dense_up,
    dense_down,
    dense_mix,
):
    seqs, width = tokens.shape
    tp = lax.axis_index("tp")
    core, chip = tp % 2, tp // 2
    half = seqs // 2
    groups = lax.axis_size("ep")
    experts = groups * expert_gate.shape[0]
    top = routes.shape[1]
    capacity = 2 * seqs * top // experts
    share_rows = seqs // lax.axis_size("tp")
    wide = share_rows * width // capacity

    swap = core * half
    hits = jnp.roll(routing(routes, experts, capacity), swap, axis=0)
    weights = jnp.roll(route_weights, swap, axis=0)
    table = jnp.any(hits, axis=1).astype(BF16).T
    pick = jnp.sum(hits * weights[:, :, None], axis=1)
    high = pick.astype(BF16)
    low = (pick - high.astype(F32)).astype(BF16)
    pick = jnp.concatenate([high, low], axis=0)
    share_at = chip * share_rows + jnp.arange(share_rows, dtype=jnp.int32)
    here = share_at[:, None] == jnp.arange(seqs, dtype=jnp.int32)[None, :]
    share = jnp.concatenate([here, here], axis=0).astype(BF16)
    place = here[:, :half].astype(F32).T

    new_state, mine, theirs = mixer(
        tokens, state, norm_gain, w_query, w_forget, w_input, w_outgate, forget_floor, head_gain, w_out
    )
    mixout = row_sum(mine, theirs)
    resid = lax.dynamic_slice_in_dim(tokens, core * half, half, 0).astype(F32) + mixout
    rows = (resid * mean_scale(resid) * ffn_gain).astype(BF16)
    packet = build(table, share, rows, core_swap(rows), wide)
    packet = packet.reshape(groups, capacity, width + wide)
    packet = lax.all_to_all(packet, "ep", split_axis=0, concat_axis=0, tiled=True)
    packet = ffn(
        packet.reshape(groups * capacity, width + wide),
        expert_gate[0],
        expert_up[0],
        expert_down[0],
        dense_gate,
        dense_up,
        dense_down,
    )
    packet = packet.reshape(groups, capacity, width + wide)
    packet = lax.all_to_all(packet, "ep", split_axis=0, concat_axis=0, tiled=True)
    mine, theirs = combine(pick, packet.reshape(groups * capacity, -1), dense_mix, place)
    mixed = (resid + row_sum(mine, theirs)).astype(BF16)
    other = core_swap(mixed)
    first = jnp.where(core == 0, mixed, other)
    second = jnp.where(core == 0, other, mixed)
    return (jnp.concatenate([first, second], axis=0), new_state)


def solution(mesh):
    in_specs = (
        P("ep", None),
        P("ep", "tp", None, None),
        P(),
        P(None, "tp"),
        P(None, "tp"),
        P(None, "tp"),
        P(None, "tp"),
        P("tp"),
        P(),
        P("tp", None),
        P(),
        P("ep", None),
        P("ep", None),
        P("ep", None, "tp"),
        P("ep", None, "tp"),
        P("ep", "tp", None),
        P(None, "ep"),
        P(None, "ep"),
        P("ep", None),
        P(),
    )
    out_specs = (P("ep", None), P("ep", "tp", None, None))
    return jax.shard_map(local, mesh=mesh, in_specs=in_specs, out_specs=out_specs, check_vma=False)
```

```python
import jax
import jax.numpy as jnp
from jax import lax
from jax.experimental import pallas as pl
from jax.experimental.pallas import tpu as pltpu
from jax.sharding import PartitionSpec as P

EPS = 1e-06
F32 = jnp.float32
BF16 = jnp.bfloat16
HBM = pl.BlockSpec(memory_space=pltpu.HBM)
VMEM = pl.BlockSpec(memory_space=pltpu.VMEM)


CHUNKS = 4


def dot(a, b):
    return jnp.dot(a, b, preferred_element_type=F32)


def dot_t(a, b):
    return lax.dot_general(a, b, (((1,), (1,)), ((), ())), preferred_element_type=F32)


def mean_scale(x):
    return lax.rsqrt(jnp.mean(x * x, axis=-1, keepdims=True) + EPS)


def sigmoid(x):
    return 1.0 / (1.0 + jnp.exp(-x))


def mixer_kernel(
    tokens_in,
    gain_in,
    floor_in,
    head_gain_in,
    state,
    w_query,
    w_forget,
    w_input,
    w_outgate,
    w_out,
    new_state,
    mine,
    theirs,
    tokens,
    gain,
    floor,
    head_gain,
    w_buf,
    wo_buf,
    held,
    keep_t,
    query_t,
    values,
    read,
    small_sem,
    w_sem,
    wo_sem,
    in_sem,
    out_sem,
):
    seqs = tokens.shape[0]
    heads, size = held.shape[1:3]
    step = seqs // CHUNKS
    core = lax.rem(lax.axis_index("tp"), 2)
    small = [
        pltpu.make_async_copy(a, b, small_sem.at[i])
        for i, (a, b) in enumerate(
            ((tokens_in, tokens), (gain_in, gain), (floor_in, floor), (head_gain_in, head_gain))
        )
    ]
    for load in small:
        load.start()
    loads = [
        pltpu.make_async_copy(w, w_buf.at[i], w_sem.at[i])
        for i, w in enumerate((w_forget, w_query, w_input, w_outgate))
    ]
    for load in loads[:3]:
        load.start()

    def fetch(j):
        rows = pl.ds(j * step, step)
        return pltpu.make_async_copy(state.at[rows], held.at[rows], in_sem.at[j])

    def flush(j):
        rows = pl.ds(j * step, step)
        return pltpu.make_async_copy(held.at[rows], new_state.at[rows], out_sem.at[j])

    for j in range(CHUNKS):
        fetch(j).start()
    loads[3].start()
    load_out = pltpu.make_async_copy(w_out, wo_buf, wo_sem)
    load_out.start()

    for load in small:
        load.wait()
    x = tokens[...].astype(F32)
    normed = (x * mean_scale(x) * gain[...]).astype(BF16)
    base = floor[...]
    loads[0].wait()
    keep = (base + (1.0 - base) * sigmoid(dot(normed, w_buf[0]))).T
    loads[1].wait()
    zq = dot(normed, w_buf[1])
    query = (zq * sigmoid(zq)).T
    for j in range(CHUNKS):
        keep_t[j, :, :] = keep[:, j * step : (j + 1) * step]
        query_t[j, :, :] = query[:, j * step : (j + 1) * step]
    loads[2].wait()
    values[...] = dot(normed, w_buf[2])

    def body(j, carry):
        fetch(j).wait()
        rows = pl.ds(pl.multiple_of(j * step, step), step)
        block = values[rows, :]
        reads = []
        for i in range(step):
            parts = []
            for h in range(heads):
                lanes = slice(h * size, (h + 1) * size)
                v = block[i : i + 1, lanes]
                k = jnp.broadcast_to(keep_t[j, lanes, i : i + 1], (size, size))
                q = jnp.broadcast_to(query_t[j, lanes, i : i + 1], (size, size))
                new = v + k * (held[j * step + i, h] - v)
                held[j * step + i, h] = new
                parts.append(jnp.sum(q * new, axis=0, keepdims=True))
            reads.append(jnp.concatenate(parts, axis=1))
        read[rows, :] = jnp.concatenate(reads, axis=0)
        flush(j).start()
        return carry

    lax.fori_loop(0, CHUNKS, body, 0)
    loads[3].wait()
    zg = dot(normed, w_buf[3])
    gate = zg * sigmoid(zg)
    outs = []
    for h in range(heads):
        lanes = slice(h * size, (h + 1) * size)
        r = read[:, lanes]
        outs.append(r * mean_scale(r) * head_gain[...] * gate[:, lanes])
    headout = jnp.concatenate(outs, axis=1).astype(BF16)
    load_out.wait()
    block = dot(headout, wo_buf[...])
    half = seqs // 2
    first = core == 0
    mine[...] = jnp.where(first, block[:half], block[half:]).astype(BF16)
    theirs[...] = jnp.where(first, block[half:], block[:half]).astype(BF16)
    for j in range(CHUNKS):
        flush(j).wait()


def mixer(tokens, state, norm_gain, w_query, w_forget, w_input, w_outgate, floor, head_gain, w_out):
    seqs, width = tokens.shape
    channels = w_query.shape[1]
    half = jax.ShapeDtypeStruct((seqs // 2, width), BF16)
    step = seqs // CHUNKS
    return pl.pallas_call(
        mixer_kernel,
        out_shape=(jax.ShapeDtypeStruct(state.shape, state.dtype), half, half),
        in_specs=[HBM] * 10,
        out_specs=(HBM, VMEM, VMEM),
        scratch_shapes=[
            pltpu.VMEM((seqs, width), BF16),
            pltpu.VMEM((1, width), F32),
            pltpu.VMEM((1, channels), F32),
            pltpu.VMEM((1, state.shape[3]), F32),
            pltpu.VMEM((4, width, channels), BF16),
            pltpu.VMEM((channels, width), BF16),
            pltpu.VMEM(state.shape, F32),
            pltpu.VMEM((CHUNKS, channels, step), F32),
            pltpu.VMEM((CHUNKS, channels, step), F32),
            pltpu.VMEM((seqs, channels), F32),
            pltpu.VMEM((seqs, channels), F32),
            pltpu.SemaphoreType.DMA((4,)),
            pltpu.SemaphoreType.DMA((4,)),
            pltpu.SemaphoreType.DMA,
            pltpu.SemaphoreType.DMA((CHUNKS,)),
            pltpu.SemaphoreType.DMA((CHUNKS,)),
        ],
        compiler_params=pltpu.CompilerParams(vmem_limit_bytes=20 << 20),
        name="mixer",
    )(
        *(
            pltpu.with_memory_space_constraint(x, pltpu.HBM)
            for x in (
                tokens,
                norm_gain.reshape(1, width),
                floor.reshape(1, channels),
                head_gain.reshape(1, -1),
                state,
                w_query,
                w_forget,
                w_input,
                w_outgate,
                w_out,
            )
        )
    )


def build_kernel(table, share, mine, other, packet):
    width = mine.shape[1]
    wide = packet.shape[1] - width
    rows = jnp.concatenate([mine[...], other[...]], axis=0)
    packet[:, :width] = dot(table[...], rows).astype(BF16)
    part = dot(share[...], rows)
    half = part.shape[0] // 2
    part = jnp.concatenate([part[:half, :wide], part[half:, wide:]], axis=0)
    copies = packet.shape[0] // part.shape[0]
    packet[:, width:] = jnp.concatenate([part] * copies, axis=0).astype(BF16)


def build(table, share, mine, other, wide):
    slots, width = table.shape[0], mine.shape[1]
    return pl.pallas_call(
        build_kernel,
        out_shape=jax.ShapeDtypeStruct((slots, width + wide), BF16),
        in_specs=[VMEM] * 4,
        out_specs=VMEM,
        compiler_params=pltpu.CompilerParams(vmem_limit_bytes=8 << 20),
        cost_estimate=pl.CostEstimate(flops=10**10, bytes_accessed=10**8, transcendentals=0),
        name="build",
    )(table, share, mine, other)


def in_group_turn(x, group):
    rows, lanes = x.shape
    x = x.reshape(rows // group, group, lanes)
    return pltpu.roll(x, group // 2, axis=1).reshape(rows, lanes)


def ffn_kernel(packet, e_gate, e_up, e_down, d_gate, d_up, d_down, out):
    width = e_gate.shape[1]
    wide = packet.shape[1] - width
    group = 8
    rows = packet[:, :width]
    gate = dot_t(rows, e_gate[...])
    upper = dot_t(rows, e_up[...])
    hidden = (gate * sigmoid(gate) * upper).astype(BF16)
    out[:, :width] = dot(hidden, e_down[...]).astype(BF16)
    share = packet[:, width:]
    gate = dot_t(share, d_gate[:, :wide]) + in_group_turn(dot_t(share, d_gate[:, wide:]), group)
    upper = dot_t(share, d_up[:, :wide]) + in_group_turn(dot_t(share, d_up[:, wide:]), group)
    hidden = (gate * sigmoid(gate) * upper).astype(BF16)
    result = dot(hidden, d_down[...])
    turned = in_group_turn(result[:, wide:], group)
    at = lax.broadcasted_iota(jnp.int32, turned.shape, 0)
    out[:, width:] = jnp.where(at % group < group // 2, result[:, :wide], turned).astype(BF16)


def ffn(packet, e_gate, e_up, e_down, d_gate, d_up, d_down):
    return pl.pallas_call(
        ffn_kernel,
        out_shape=jax.ShapeDtypeStruct(packet.shape, BF16),
        in_specs=[VMEM] * 7,
        out_specs=VMEM,
        compiler_params=pltpu.CompilerParams(vmem_limit_bytes=32 << 20),
        name="ffn",
    )(packet, e_gate, e_up, e_down, d_gate, d_up, d_down)


def combine_kernel(pick, packet, mix, place, mine, theirs):
    width = mix.shape[1]
    wide = packet.shape[1] - width
    half = mine.shape[0]
    group = 8
    moe = dot(pick[...], packet[:, :width])
    moe = moe[: 2 * half] + moe[2 * half :]
    parts = packet[:, width:].astype(F32)
    parts = jnp.sum(parts.reshape(-1, group, wide), axis=0)
    dense = jnp.concatenate([parts[: group // 2], parts[group // 2 :]], axis=1)
    dense = sigmoid(mix[...]) * dense
    total = moe[:half]
    where = place[...]
    for r in range(group // 2):
        total = total + where[:, r : r + 1] * dense[r : r + 1]
    mine[...] = total.astype(BF16)
    theirs[...] = moe[half:].astype(BF16)


def combine(pick, packet, mix, place):
    width = mix.shape[0]
    half = jax.ShapeDtypeStruct((pick.shape[0] // 4, width), BF16)
    return pl.pallas_call(
        combine_kernel,
        out_shape=(half, half),
        in_specs=[VMEM] * 4,
        out_specs=(VMEM, VMEM),
        compiler_params=pltpu.CompilerParams(vmem_limit_bytes=8 << 20),
        name="combine",
    )(pick, packet, mix.reshape(1, width), place)


def routing(local_routes, experts, capacity):
    flat = local_routes.reshape(-1)
    onehot = (flat[:, None] == jnp.arange(experts, dtype=jnp.int32)[None, :]).astype(jnp.int32)
    before = jnp.cumsum(onehot, axis=0) - onehot
    slot = jnp.sum(before * onehot, axis=1)
    where = (flat * capacity + slot).reshape(local_routes.shape)
    return where[:, :, None] == jnp.arange(experts * capacity, dtype=jnp.int32)[None, None, :]


def core_swap(x):
    return lax.ppermute(x, "tp", [(t, t ^ 1) for t in range(8)])


def added(mine, other):
    return (mine.astype(F32) + other.astype(F32)).astype(BF16)


def first_turn(mine):
    return lax.ppermute(mine, "tp", [(t, t ^ 2) for t in range(8)])


def second_turn(mine):
    return lax.ppermute(mine, "tp", [(t, (6 - t // 2 * 2) + t % 2) for t in range(8)])


def tables(routes, route_weights, core, chip, share_rows, experts, capacity):
    seqs = routes.shape[0]
    half = seqs // 2
    swap = core * half
    hits = jnp.roll(routing(routes, experts, capacity), swap, axis=0)
    weights = jnp.roll(route_weights, swap, axis=0)
    table = jnp.any(hits, axis=1).astype(BF16).T
    pick = jnp.sum(hits * weights[:, :, None], axis=1)
    high = pick.astype(BF16)
    low = (pick - high.astype(F32)).astype(BF16)
    pick = jnp.concatenate([high, low], axis=0)
    share_at = chip * share_rows + jnp.arange(share_rows, dtype=jnp.int32)
    here = share_at[:, None] == jnp.arange(seqs, dtype=jnp.int32)[None, :]
    share = jnp.concatenate([here, here], axis=0).astype(BF16)
    return table, pick, share, here[:, :half].astype(F32).T


def local(
    tokens,
    state,
    norm_gain,
    w_query,
    w_forget,
    w_input,
    w_outgate,
    forget_floor,
    head_gain,
    w_out,
    ffn_gain,
    routes,
    route_weights,
    expert_gate,
    expert_up,
    expert_down,
    dense_gate,
    dense_up,
    dense_down,
    dense_mix,
):
    seqs, width = tokens.shape
    tp = lax.axis_index("tp")
    core, chip = tp % 2, tp // 2
    half = seqs // 2
    groups = lax.axis_size("ep")
    experts = groups * expert_gate.shape[0]
    top = routes.shape[1]
    capacity = 2 * seqs * top // experts
    share_rows = seqs // lax.axis_size("tp")
    wide = share_rows * width // capacity

    new_state, mine, theirs = mixer(
        tokens, state, norm_gain, w_query, w_forget, w_input, w_outgate, forget_floor, head_gain, w_out
    )
    mine = added(mine, core_swap(theirs))
    mine, routes, route_weights = lax.optimization_barrier((mine, routes, route_weights))
    matrices = tables(routes, route_weights, core, chip, share_rows, experts, capacity)
    mine = added(mine, first_turn(mine))
    other, *matrices = lax.optimization_barrier((second_turn(mine), *matrices))
    table, pick, share, place = matrices
    mixout = mine.astype(F32) + other.astype(F32)
    resid = lax.dynamic_slice_in_dim(tokens, core * half, half, 0).astype(F32) + mixout
    rows = (resid * mean_scale(resid) * ffn_gain).astype(BF16)
    packet = build(table, share, rows, core_swap(rows), wide)
    packet = packet.reshape(groups, capacity, width + wide)
    packet = lax.all_to_all(packet, "ep", split_axis=0, concat_axis=0, tiled=True)
    packet = ffn(
        packet.reshape(groups * capacity, width + wide),
        expert_gate[0].T,
        expert_up[0].T,
        expert_down[0],
        dense_gate.T,
        dense_up.T,
        dense_down,
    )
    packet = packet.reshape(groups, capacity, width + wide)
    packet = lax.all_to_all(packet, "ep", split_axis=0, concat_axis=0, tiled=True)
    mine, theirs = combine(pick, packet.reshape(groups * capacity, -1), dense_mix, place)
    mine = added(mine, core_swap(theirs))
    mine = added(mine, first_turn(mine))
    total = mine.astype(F32) + second_turn(mine).astype(F32)
    mixed = (resid + total).astype(BF16)
    other = core_swap(mixed)
    first = jnp.where(core == 0, mixed, other)
    second = jnp.where(core == 0, other, mixed)
    return (jnp.concatenate([first, second], axis=0), new_state)


def solution(mesh):
    in_specs = (
        P("ep", None),
        P("ep", "tp", None, None),
        P(),
        P(None, "tp"),
        P(None, "tp"),
        P(None, "tp"),
        P(None, "tp"),
        P("tp"),
        P(),
        P("tp", None),
        P(),
        P("ep", None),
        P("ep", None),
        P("ep", None, "tp"),
        P("ep", None, "tp"),
        P("ep", "tp", None),
        P(None, "ep"),
        P(None, "ep"),
        P("ep", None),
        P(),
    )
    out_specs = (P("ep", None), P("ep", "tp", None, None))
    return jax.shard_map(local, mesh=mesh, in_specs=in_specs, out_specs=out_specs, check_vma=False)
```

```python
import jax
import jax.numpy as jnp
from jax import lax
from jax.experimental import pallas as pl
from jax.experimental.pallas import tpu as pltpu
from jax.sharding import PartitionSpec as P

EPS = 1e-06
F32 = jnp.float32
BF16 = jnp.bfloat16
HBM = pl.BlockSpec(memory_space=pltpu.HBM)
VMEM = pl.BlockSpec(memory_space=pltpu.VMEM)


CHUNKS = 4


def dot(a, b):
    return jnp.dot(a, b, preferred_element_type=F32)


def dot_t(a, b):
    return lax.dot_general(a, b, (((1,), (1,)), ((), ())), preferred_element_type=F32)


def mean_scale(x):
    return lax.rsqrt(jnp.mean(x * x, axis=-1, keepdims=True) + EPS)


def sigmoid(x):
    return 1.0 / (1.0 + jnp.exp(-x))


def mixer_kernel(
    tokens_in,
    gain_in,
    floor_in,
    head_gain_in,
    state,
    w_query,
    w_forget,
    w_input,
    w_outgate,
    w_out,
    new_state,
    mine,
    theirs,
    tokens,
    gain,
    floor,
    head_gain,
    w_buf,
    wo_buf,
    held,
    spread,
    columns,
    values,
    read,
    small_sem,
    w_sem,
    wo_sem,
    in_sem,
    out_sem,
):
    seqs = tokens.shape[0]
    heads, size = held.shape[1:3]
    step = seqs // CHUNKS
    core = lax.rem(lax.axis_index("tp"), 2)
    small = [
        pltpu.make_async_copy(a, b, small_sem.at[i])
        for i, (a, b) in enumerate(
            ((tokens_in, tokens), (gain_in, gain), (floor_in, floor), (head_gain_in, head_gain))
        )
    ]
    for load in small:
        load.start()
    loads = [
        pltpu.make_async_copy(w, w_buf.at[i], w_sem.at[i])
        for i, w in enumerate((w_forget, w_query, w_input, w_outgate))
    ]
    for load in loads[:3]:
        load.start()

    def fetch(j):
        rows = pl.ds(j * step, step)
        return pltpu.make_async_copy(state.at[rows], held.at[rows], in_sem.at[j])

    def flush(j):
        rows = pl.ds(j * step, step)
        return pltpu.make_async_copy(held.at[rows], new_state.at[rows], out_sem.at[j])

    for load in small:
        load.wait()
    x = tokens[...].astype(F32)
    normed = (x * mean_scale(x) * gain[...]).astype(BF16)
    base = floor[...]
    row = lax.broadcasted_iota(jnp.int32, spread.shape[1:], 0)
    lane = lax.broadcasted_iota(jnp.int32, spread.shape[1:], 1)
    source = jnp.where(row < 3 * seqs, row % seqs - lane // size, -1)
    for p in range(spread.shape[0]):
        spread[p] = jnp.where(source == 2 * p, 1.0, 0.0).astype(BF16)
    loads[0].wait()
    for j in range(CHUNKS):
        fetch(j).start()
    loads[3].start()
    load_out = pltpu.make_async_copy(w_out, wo_buf, wo_sem)
    load_out.start()
    keep = base + (1.0 - base) * sigmoid(dot(normed, w_buf[0]))
    loads[1].wait()
    zq = dot(normed, w_buf[1])
    both = jnp.concatenate([keep, zq * sigmoid(zq)], axis=1)
    parts = []
    for _ in range(3):
        parts.append(both.astype(BF16).astype(F32))
        both = both - parts[-1]
    parts.append(jnp.zeros((size - 3 * seqs, both.shape[1]), F32))
    columns[...] = jnp.concatenate(parts, axis=0).T.astype(BF16)
    loads[2].wait()
    values[...] = dot(normed, w_buf[2])

    def body(j, carry):
        fetch(j).wait()
        rows = pl.ds(pl.multiple_of(j * step, step), step)
        block = values[rows, :]
        reads = [[None] * heads for _ in range(step)]
        for p in range(step // 2):
            one = spread[j * (step // 2) + p]
            for h in range(heads):
                at = h * size
                keeps = dot(columns[at : at + size, :], one)
                queries = dot(columns[(heads + h) * size : (heads + h + 1) * size, :], one)
                for i in range(2):
                    t = 2 * p + i
                    v = block[t : t + 1, at : at + size]
                    lanes = slice(i * size, (i + 1) * size)
                    new = v + keeps[:, lanes] * (held[j * step + t, h] - v)
                    held[j * step + t, h] = new
                    reads[t][h] = jnp.sum(queries[:, lanes] * new, axis=0, keepdims=True)
        read[rows, :] = jnp.concatenate([jnp.concatenate(r, axis=1) for r in reads], axis=0)
        flush(j).start()
        return carry

    lax.fori_loop(0, CHUNKS, body, 0)
    loads[3].wait()
    zg = dot(normed, w_buf[3])
    gate = zg * sigmoid(zg)
    outs = []
    for h in range(heads):
        lanes = slice(h * size, (h + 1) * size)
        r = read[:, lanes]
        outs.append(r * mean_scale(r) * head_gain[...] * gate[:, lanes])
    headout = jnp.concatenate(outs, axis=1).astype(BF16)
    load_out.wait()
    block = dot(headout, wo_buf[...])
    half = seqs // 2
    first = core == 0
    mine[...] = jnp.where(first, block[:half], block[half:]).astype(BF16)
    theirs[...] = jnp.where(first, block[half:], block[:half]).astype(BF16)
    for j in range(CHUNKS):
        flush(j).wait()


def mixer(tokens, state, norm_gain, w_query, w_forget, w_input, w_outgate, floor, head_gain, w_out):
    seqs, width = tokens.shape
    channels = w_query.shape[1]
    half = jax.ShapeDtypeStruct((seqs // 2, width), BF16)
    size = state.shape[3]
    return pl.pallas_call(
        mixer_kernel,
        out_shape=(jax.ShapeDtypeStruct(state.shape, state.dtype), half, half),
        in_specs=[HBM] * 10,
        out_specs=(HBM, VMEM, VMEM),
        scratch_shapes=[
            pltpu.VMEM((seqs, width), BF16),
            pltpu.VMEM((1, width), F32),
            pltpu.VMEM((1, channels), F32),
            pltpu.VMEM((1, state.shape[3]), F32),
            pltpu.VMEM((4, width, channels), BF16),
            pltpu.VMEM((channels, width), BF16),
            pltpu.VMEM(state.shape, F32),
            pltpu.VMEM((seqs // 2, size, 2 * size), BF16),
            pltpu.VMEM((2 * channels, size), BF16),
            pltpu.VMEM((seqs, channels), F32),
            pltpu.VMEM((seqs, channels), F32),
            pltpu.SemaphoreType.DMA((4,)),
            pltpu.SemaphoreType.DMA((4,)),
            pltpu.SemaphoreType.DMA,
            pltpu.SemaphoreType.DMA((CHUNKS,)),
            pltpu.SemaphoreType.DMA((CHUNKS,)),
        ],
        compiler_params=pltpu.CompilerParams(vmem_limit_bytes=20 << 20),
        name="mixer",
    )(
        *(
            pltpu.with_memory_space_constraint(x, pltpu.HBM)
            for x in (
                tokens,
                norm_gain.reshape(1, width),
                floor.reshape(1, channels),
                head_gain.reshape(1, -1),
                state,
                w_query,
                w_forget,
                w_input,
                w_outgate,
                w_out,
            )
        )
    )


def build_kernel(table, share, mine, other, packet):
    width = mine.shape[1]
    wide = packet.shape[1] - width
    rows = jnp.concatenate([mine[...], other[...]], axis=0)
    packet[:, :width] = dot(table[...], rows).astype(BF16)
    part = dot(share[...], rows)
    half = part.shape[0] // 2
    part = jnp.concatenate([part[:half, :wide], part[half:, wide:]], axis=0)
    copies = packet.shape[0] // part.shape[0]
    packet[:, width:] = jnp.concatenate([part] * copies, axis=0).astype(BF16)


def build(table, share, mine, other, wide):
    slots, width = table.shape[0], mine.shape[1]
    return pl.pallas_call(
        build_kernel,
        out_shape=jax.ShapeDtypeStruct((slots, width + wide), BF16),
        in_specs=[VMEM] * 4,
        out_specs=VMEM,
        compiler_params=pltpu.CompilerParams(vmem_limit_bytes=8 << 20),
        cost_estimate=pl.CostEstimate(flops=10**10, bytes_accessed=10**8, transcendentals=0),
        name="build",
    )(table, share, mine, other)


def in_group_turn(x, group):
    rows, lanes = x.shape
    x = x.reshape(rows // group, group, lanes)
    return pltpu.roll(x, group // 2, axis=1).reshape(rows, lanes)


def ffn_kernel(packet, e_gate, e_up, e_down, d_gate, d_up, d_down, out):
    width = e_gate.shape[1]
    wide = packet.shape[1] - width
    group = 8
    rows = packet[:, :width]
    gate = dot_t(rows, e_gate[...])
    upper = dot_t(rows, e_up[...])
    hidden = (gate * sigmoid(gate) * upper).astype(BF16)
    out[:, :width] = dot(hidden, e_down[...]).astype(BF16)
    share = packet[:, width:]
    gate = dot_t(share, d_gate[:, :wide]) + in_group_turn(dot_t(share, d_gate[:, wide:]), group)
    upper = dot_t(share, d_up[:, :wide]) + in_group_turn(dot_t(share, d_up[:, wide:]), group)
    hidden = (gate * sigmoid(gate) * upper).astype(BF16)
    result = dot(hidden, d_down[...])
    turned = in_group_turn(result[:, wide:], group)
    at = lax.broadcasted_iota(jnp.int32, turned.shape, 0)
    out[:, width:] = jnp.where(at % group < group // 2, result[:, :wide], turned).astype(BF16)


def ffn(packet, e_gate, e_up, e_down, d_gate, d_up, d_down):
    return pl.pallas_call(
        ffn_kernel,
        out_shape=jax.ShapeDtypeStruct(packet.shape, BF16),
        in_specs=[VMEM] * 7,
        out_specs=VMEM,
        compiler_params=pltpu.CompilerParams(vmem_limit_bytes=32 << 20),
        name="ffn",
    )(packet, e_gate, e_up, e_down, d_gate, d_up, d_down)


def combine_kernel(pick, packet, mix, place, mine, theirs):
    width = mix.shape[1]
    wide = packet.shape[1] - width
    half = mine.shape[0]
    group = 8
    moe = dot(pick[...], packet[:, :width])
    moe = moe[: 2 * half] + moe[2 * half :]
    parts = packet[:, width:].astype(F32)
    parts = jnp.sum(parts.reshape(-1, group, wide), axis=0)
    dense = jnp.concatenate([parts[: group // 2], parts[group // 2 :]], axis=1)
    dense = sigmoid(mix[...]) * dense
    total = moe[:half]
    where = place[...]
    for r in range(group // 2):
        total = total + where[:, r : r + 1] * dense[r : r + 1]
    mine[...] = total.astype(BF16)
    theirs[...] = moe[half:].astype(BF16)


def combine(pick, packet, mix, place):
    width = mix.shape[0]
    half = jax.ShapeDtypeStruct((pick.shape[0] // 4, width), BF16)
    return pl.pallas_call(
        combine_kernel,
        out_shape=(half, half),
        in_specs=[VMEM] * 4,
        out_specs=(VMEM, VMEM),
        compiler_params=pltpu.CompilerParams(vmem_limit_bytes=8 << 20),
        name="combine",
    )(pick, packet, mix.reshape(1, width), place)


def routing(local_routes, experts, capacity):
    flat = local_routes.reshape(-1)
    onehot = (flat[:, None] == jnp.arange(experts, dtype=jnp.int32)[None, :]).astype(jnp.int32)
    before = jnp.cumsum(onehot, axis=0) - onehot
    slot = jnp.sum(before * onehot, axis=1)
    where = (flat * capacity + slot).reshape(local_routes.shape)
    return where[:, :, None] == jnp.arange(experts * capacity, dtype=jnp.int32)[None, None, :]


def core_swap(x):
    return lax.ppermute(x, "tp", [(t, t ^ 1) for t in range(8)])


def added(mine, other):
    return (mine.astype(F32) + other.astype(F32)).astype(BF16)


def from_chips(mine):
    return [lax.ppermute(mine, "tp", [(t, t ^ d) for t in range(8)]) for d in (4, 2, 6)]


def chip_sum(mine, far, near, across):
    return (mine.astype(F32) + near.astype(F32)) + (far.astype(F32) + across.astype(F32))


def tables(routes, route_weights, core, chip, share_rows, experts, capacity):
    seqs = routes.shape[0]
    half = seqs // 2
    swap = core * half
    hits = jnp.roll(routing(routes, experts, capacity), swap, axis=0)
    weights = jnp.roll(route_weights, swap, axis=0)
    table = jnp.any(hits, axis=1).astype(BF16).T
    pick = jnp.sum(hits * weights[:, :, None], axis=1)
    high = pick.astype(BF16)
    low = (pick - high.astype(F32)).astype(BF16)
    pick = jnp.concatenate([high, low], axis=0)
    share_at = chip * share_rows + jnp.arange(share_rows, dtype=jnp.int32)
    here = share_at[:, None] == jnp.arange(seqs, dtype=jnp.int32)[None, :]
    share = jnp.concatenate([here, here], axis=0).astype(BF16)
    return table, pick, share, here[:, :half].astype(F32).T


def local(
    tokens,
    state,
    norm_gain,
    w_query,
    w_forget,
    w_input,
    w_outgate,
    forget_floor,
    head_gain,
    w_out,
    ffn_gain,
    routes,
    route_weights,
    expert_gate,
    expert_up,
    expert_down,
    dense_gate,
    dense_up,
    dense_down,
    dense_mix,
):
    seqs, width = tokens.shape
    tp = lax.axis_index("tp")
    core, chip = tp % 2, tp // 2
    half = seqs // 2
    groups = lax.axis_size("ep")
    experts = groups * expert_gate.shape[0]
    top = routes.shape[1]
    capacity = 2 * seqs * top // experts
    share_rows = seqs // lax.axis_size("tp")
    wide = share_rows * width // capacity

    new_state, mine, theirs = mixer(
        tokens, state, norm_gain, w_query, w_forget, w_input, w_outgate, forget_floor, head_gain, w_out
    )
    mine = added(mine, core_swap(theirs))
    mine, routes, route_weights = lax.optimization_barrier((mine, routes, route_weights))
    matrices = tables(routes, route_weights, core, chip, share_rows, experts, capacity)
    *others, table, pick, share, place = lax.optimization_barrier((*from_chips(mine), *matrices))
    mixout = chip_sum(mine, *others)
    resid = lax.dynamic_slice_in_dim(tokens, core * half, half, 0).astype(F32) + mixout
    rows = (resid * mean_scale(resid) * ffn_gain).astype(BF16)
    packet = build(table, share, rows, core_swap(rows), wide)
    packet = packet.reshape(groups, capacity, width + wide)
    packet = lax.all_to_all(packet, "ep", split_axis=0, concat_axis=0, tiled=True)
    packet = ffn(
        packet.reshape(groups * capacity, width + wide),
        expert_gate[0].T,
        expert_up[0].T,
        expert_down[0],
        dense_gate.T,
        dense_up.T,
        dense_down,
    )
    packet = packet.reshape(groups, capacity, width + wide)
    packet = lax.all_to_all(packet, "ep", split_axis=0, concat_axis=0, tiled=True)
    mine, theirs = combine(pick, packet.reshape(groups * capacity, -1), dense_mix, place)
    mine = added(mine, core_swap(theirs))
    mixed = (resid + chip_sum(mine, *from_chips(mine))).astype(BF16)
    other = core_swap(mixed)
    first = jnp.where(core == 0, mixed, other)
    second = jnp.where(core == 0, other, mixed)
    return (jnp.concatenate([first, second], axis=0), new_state)


def solution(mesh):
    in_specs = (
        P("ep", None),
        P("ep", "tp", None, None),
        P(),
        P(None, "tp"),
        P(None, "tp"),
        P(None, "tp"),
        P(None, "tp"),
        P("tp"),
        P(),
        P("tp", None),
        P(),
        P("ep", None),
        P("ep", None),
        P("ep", None, "tp"),
        P("ep", None, "tp"),
        P("ep", "tp", None),
        P(None, "ep"),
        P(None, "ep"),
        P("ep", None),
        P(),
    )
    out_specs = (P("ep", None), P("ep", "tp", None, None))
    return jax.shard_map(local, mesh=mesh, in_specs=in_specs, out_specs=out_specs, check_vma=False)
```

```python
import jax
import jax.numpy as jnp
from jax import lax
from jax.experimental import pallas as pl
from jax.experimental.pallas import tpu as pltpu
from jax.sharding import PartitionSpec as P

EPS = 1e-06
F32 = jnp.float32
BF16 = jnp.bfloat16
HBM = pl.BlockSpec(memory_space=pltpu.HBM)
VMEM = pl.BlockSpec(memory_space=pltpu.VMEM)


CHUNKS = 4


def dot(a, b):
    return jnp.dot(a, b, preferred_element_type=F32)


def dot_t(a, b):
    return lax.dot_general(a, b, (((1,), (1,)), ((), ())), preferred_element_type=F32)


def mean_scale(x):
    return lax.rsqrt(jnp.mean(x * x, axis=-1, keepdims=True) + EPS)


def sigmoid(x):
    return 1.0 / (1.0 + jnp.exp(-x))


def mixer_kernel(
    tokens_in,
    gain_in,
    floor_in,
    head_gain_in,
    state,
    w_query,
    w_forget,
    w_input,
    w_outgate,
    w_out,
    new_state,
    mine,
    theirs,
    tokens,
    gain,
    floor,
    head_gain,
    w_buf,
    wo_buf,
    held,
    spread,
    columns,
    values,
    read,
    small_sem,
    w_sem,
    wo_sem,
    in_sem,
    out_sem,
):
    seqs = tokens.shape[0]
    heads, size = held.shape[1:3]
    step = seqs // CHUNKS
    core = lax.rem(lax.axis_index("tp"), 2)
    small = [
        pltpu.make_async_copy(a, b, small_sem.at[i])
        for i, (a, b) in enumerate(
            ((tokens_in, tokens), (gain_in, gain), (floor_in, floor), (head_gain_in, head_gain))
        )
    ]
    for load in small:
        load.start()
    loads = [
        pltpu.make_async_copy(w, w_buf.at[i], w_sem.at[i])
        for i, w in enumerate((w_forget, w_query, w_input, w_outgate))
    ]
    for load in loads[:3]:
        load.start()

    def fetch(j):
        rows = pl.ds(j * step, step)
        return pltpu.make_async_copy(state.at[rows], held.at[rows], in_sem.at[j])

    def flush(j):
        rows = pl.ds(j * step, step)
        return pltpu.make_async_copy(held.at[rows], new_state.at[rows], out_sem.at[j])

    for load in small[:2]:
        load.wait()
    x = tokens[...].astype(F32)
    normed = (x * mean_scale(x) * gain[...]).astype(BF16)
    for j in range(2):
        fetch(j).start()
    for load in small[2:]:
        load.wait()
    base = floor[...]
    row = lax.broadcasted_iota(jnp.int32, spread.shape[1:], 0)
    lane = lax.broadcasted_iota(jnp.int32, spread.shape[1:], 1)
    source = jnp.where(row < 3 * seqs, row % seqs - lane // size, -1)
    for p in range(spread.shape[0]):
        spread[p] = jnp.where(source == 2 * p, 1.0, 0.0).astype(BF16)
    loads[0].wait()
    for j in range(2, CHUNKS):
        fetch(j).start()
    keep = base + (1.0 - base) * sigmoid(dot(normed, w_buf[0]))
    loads[1].wait()
    loads[3].start()
    load_out = pltpu.make_async_copy(w_out, wo_buf, wo_sem)
    load_out.start()
    zq = dot(normed, w_buf[1])
    both = jnp.concatenate([keep, zq * sigmoid(zq)], axis=1)
    parts = []
    for _ in range(3):
        parts.append(both.astype(BF16).astype(F32))
        both = both - parts[-1]
    parts.append(jnp.zeros((size - 3 * seqs, both.shape[1]), F32))
    columns[...] = jnp.concatenate(parts, axis=0).T.astype(BF16)
    loads[2].wait()
    values[...] = dot(normed, w_buf[2])

    def body(j, carry):
        fetch(j).wait()
        rows = pl.ds(pl.multiple_of(j * step, step), step)
        block = values[rows, :]
        reads = [[None] * heads for _ in range(step)]
        for p in range(step // 2):
            one = spread[j * (step // 2) + p]
            for h in range(heads):
                at = h * size
                keeps = dot(columns[at : at + size, :], one)
                queries = dot(columns[(heads + h) * size : (heads + h + 1) * size, :], one)
                for i in range(2):
                    t = 2 * p + i
                    v = block[t : t + 1, at : at + size]
                    lanes = slice(i * size, (i + 1) * size)
                    new = v + keeps[:, lanes] * (held[j * step + t, h] - v)
                    held[j * step + t, h] = new
                    reads[t][h] = jnp.sum(queries[:, lanes] * new, axis=0, keepdims=True)
        read[rows, :] = jnp.concatenate([jnp.concatenate(r, axis=1) for r in reads], axis=0)
        flush(j).start()
        return carry

    lax.fori_loop(0, CHUNKS, body, 0)
    loads[3].wait()
    zg = dot(normed, w_buf[3])
    gate = zg * sigmoid(zg)
    outs = []
    for h in range(heads):
        lanes = slice(h * size, (h + 1) * size)
        r = read[:, lanes]
        outs.append(r * mean_scale(r) * head_gain[...] * gate[:, lanes])
    headout = jnp.concatenate(outs, axis=1).astype(BF16)
    load_out.wait()
    block = dot(headout, wo_buf[...])
    half = seqs // 2
    first = core == 0
    mine[...] = jnp.where(first, block[:half], block[half:]).astype(BF16)
    theirs[...] = jnp.where(first, block[half:], block[:half]).astype(BF16)
    for j in range(CHUNKS):
        flush(j).wait()


def mixer(tokens, state, norm_gain, w_query, w_forget, w_input, w_outgate, floor, head_gain, w_out):
    seqs, width = tokens.shape
    channels = w_query.shape[1]
    half = jax.ShapeDtypeStruct((seqs // 2, width), BF16)
    size = state.shape[3]
    return pl.pallas_call(
        mixer_kernel,
        out_shape=(jax.ShapeDtypeStruct(state.shape, state.dtype), half, half),
        in_specs=[HBM] * 10,
        out_specs=(HBM, VMEM, VMEM),
        scratch_shapes=[
            pltpu.VMEM((seqs, width), BF16),
            pltpu.VMEM((1, width), F32),
            pltpu.VMEM((1, channels), F32),
            pltpu.VMEM((1, state.shape[3]), F32),
            pltpu.VMEM((4, width, channels), BF16),
            pltpu.VMEM((channels, width), BF16),
            pltpu.VMEM(state.shape, F32),
            pltpu.VMEM((seqs // 2, size, 2 * size), BF16),
            pltpu.VMEM((2 * channels, size), BF16),
            pltpu.VMEM((seqs, channels), F32),
            pltpu.VMEM((seqs, channels), F32),
            pltpu.SemaphoreType.DMA((4,)),
            pltpu.SemaphoreType.DMA((4,)),
            pltpu.SemaphoreType.DMA,
            pltpu.SemaphoreType.DMA((CHUNKS,)),
            pltpu.SemaphoreType.DMA((CHUNKS,)),
        ],
        compiler_params=pltpu.CompilerParams(vmem_limit_bytes=20 << 20),
        name="mixer",
    )(
        *(
            pltpu.with_memory_space_constraint(x, pltpu.HBM)
            for x in (
                tokens,
                norm_gain.reshape(1, width),
                floor.reshape(1, channels),
                head_gain.reshape(1, -1),
                state,
                w_query,
                w_forget,
                w_input,
                w_outgate,
                w_out,
            )
        )
    )


def build_kernel(table, mine, other, packet):
    rows = jnp.concatenate([mine[...], other[...]], axis=0)
    packet[...] = dot(table[...], rows).astype(BF16)


def build(table, mine, other):
    return pl.pallas_call(
        build_kernel,
        out_shape=jax.ShapeDtypeStruct((table.shape[0], mine.shape[1]), BF16),
        in_specs=[VMEM] * 3,
        out_specs=VMEM,
        compiler_params=pltpu.CompilerParams(vmem_limit_bytes=8 << 20),
        cost_estimate=pl.CostEstimate(flops=10**10, bytes_accessed=10**8, transcendentals=0),
        name="build",
    )(table, mine, other)


def own_slots(shape, group, core):
    at = lax.broadcasted_iota(jnp.int32, shape, 0)
    return (at % group) // (group // 2) == core


def in_group_turn(x, group):
    rows, lanes = x.shape
    x = x.reshape(rows // group, group, lanes)
    return pltpu.roll(x, group // 2, axis=1).reshape(rows, lanes)


def dense_kernel(packet, gate_w, up_w, down_w, out):
    wide = out.shape[1]
    group = 8
    core = lax.rem(lax.axis_index("tp"), 2)
    share = packet[...]
    gate = dot_t(share, gate_w[...])
    upper = dot_t(share, up_w[...])
    hidden = (gate * sigmoid(gate) * upper).astype(BF16)
    result = dot(hidden, down_w[...])
    turned = in_group_turn(result[:, wide:], group)
    own = own_slots(turned.shape, group, core)
    out[...] = jnp.where(own, turned, result[:, :wide]).astype(BF16)


def dense_share(packet, gate_w, up_w, down_w):
    rows, width = packet.shape
    return pl.pallas_call(
        dense_kernel,
        out_shape=jax.ShapeDtypeStruct((rows, width // 2), BF16),
        in_specs=[VMEM] * 4,
        out_specs=VMEM,
        compiler_params=pltpu.CompilerParams(vmem_limit_bytes=16 << 20),
        name="dense",
    )(packet, gate_w, up_w, down_w)


def ffn_kernel(packet, other, share, e_gate, e_up, e_down, out):
    width = packet.shape[1]
    core = lax.rem(lax.axis_index("tp"), 2)
    own = own_slots(packet.shape, 8, core)
    rows = jnp.where(own, packet[...].astype(F32), other[...].astype(F32)).astype(BF16)
    gate = dot_t(rows, e_gate[...])
    upper = dot_t(rows, e_up[...])
    hidden = (gate * sigmoid(gate) * upper).astype(BF16)
    out[:, :width] = dot(hidden, e_down[...]).astype(BF16)
    out[:, width:] = share[...]


def ffn(packet, other, share, e_gate, e_up, e_down):
    rows, width = packet.shape
    return pl.pallas_call(
        ffn_kernel,
        out_shape=jax.ShapeDtypeStruct((rows, width + share.shape[1]), BF16),
        in_specs=[VMEM] * 6,
        out_specs=VMEM,
        compiler_params=pltpu.CompilerParams(vmem_limit_bytes=24 << 20),
        name="ffn",
    )(packet, other, share, e_gate, e_up, e_down)


def combine_kernel(pick, packet, mix, place, mine, theirs):
    width = mix.shape[1]
    wide = packet.shape[1] - width
    half = mine.shape[0]
    group = 8
    moe = dot(pick[...], packet[:, :width])
    moe = moe[: 2 * half] + moe[2 * half :]
    parts = packet[:, width:].astype(F32)
    parts = jnp.sum(parts.reshape(-1, group, wide), axis=0)
    upper, lower = parts[: group // 2], parts[group // 2 :]
    first = lax.rem(lax.axis_index("tp"), 2) == 0
    dense = jnp.concatenate(
        [jnp.where(first, lower, upper), jnp.where(first, upper, lower)], axis=1
    )
    dense = sigmoid(mix[...]) * dense
    total = moe[:half]
    where = place[...]
    for r in range(group // 2):
        total = total + where[:, r : r + 1] * dense[r : r + 1]
    mine[...] = total.astype(BF16)
    theirs[...] = moe[half:].astype(BF16)


def combine(pick, packet, mix, place):
    width = mix.shape[0]
    half = jax.ShapeDtypeStruct((pick.shape[0] // 4, width), BF16)
    return pl.pallas_call(
        combine_kernel,
        out_shape=(half, half),
        in_specs=[VMEM] * 4,
        out_specs=(VMEM, VMEM),
        compiler_params=pltpu.CompilerParams(vmem_limit_bytes=8 << 20),
        name="combine",
    )(pick, packet, mix.reshape(1, width), place)


def routing(local_routes, experts, capacity):
    flat = local_routes.reshape(-1)
    onehot = (flat[:, None] == jnp.arange(experts, dtype=jnp.int32)[None, :]).astype(jnp.int32)
    before = jnp.cumsum(onehot, axis=0) - onehot
    slot = jnp.sum(before * onehot, axis=1)
    where = (flat * capacity + slot).reshape(local_routes.shape)
    return where[:, :, None] == jnp.arange(experts * capacity, dtype=jnp.int32)[None, None, :]


def core_swap(x):
    return lax.ppermute(x, "tp", [(t, t ^ 1) for t in range(8)])


def added(mine, other):
    return (mine.astype(F32) + other.astype(F32)).astype(BF16)


def from_chips(mine):
    return [lax.ppermute(mine, "tp", [(t, t ^ d) for t in range(8)]) for d in (4, 2, 6)]


def chip_sum(mine, far, near, across):
    return (mine.astype(F32) + near.astype(F32)) + (far.astype(F32) + across.astype(F32))


def tables(routes, route_weights, core, chip, share_rows, experts, capacity):
    seqs = routes.shape[0]
    half = seqs // 2
    swap = core * half
    hits = jnp.roll(routing(routes, experts, capacity), swap, axis=0)
    weights = jnp.roll(route_weights, swap, axis=0)
    slots = jnp.any(hits, axis=1)
    pick = jnp.sum(hits * weights[:, :, None], axis=1)
    high = pick.astype(BF16)
    low = (pick - high.astype(F32)).astype(BF16)
    pick = jnp.concatenate([high, low], axis=0)
    share_at = chip * share_rows + jnp.arange(share_rows, dtype=jnp.int32)
    here = share_at[:, None] == jnp.arange(seqs, dtype=jnp.int32)[None, :]
    share = jnp.tile(here, (slots.shape[1] // share_rows, 1))
    own = own_slots((slots.shape[1], seqs), capacity, core)
    table = jnp.where(own, slots.T, share).astype(BF16)
    return table, pick, here[:, :half].astype(F32).T


def local(
    tokens,
    state,
    norm_gain,
    w_query,
    w_forget,
    w_input,
    w_outgate,
    forget_floor,
    head_gain,
    w_out,
    ffn_gain,
    routes,
    route_weights,
    expert_gate,
    expert_up,
    expert_down,
    dense_gate,
    dense_up,
    dense_down,
    dense_mix,
):
    seqs, width = tokens.shape
    tp = lax.axis_index("tp")
    core, chip = tp % 2, tp // 2
    half = seqs // 2
    groups = lax.axis_size("ep")
    experts = groups * expert_gate.shape[0]
    top = routes.shape[1]
    capacity = 2 * seqs * top // experts
    share_rows = seqs // lax.axis_size("tp")
    wide = share_rows * width // capacity

    new_state, mine, theirs = mixer(
        tokens, state, norm_gain, w_query, w_forget, w_input, w_outgate, forget_floor, head_gain, w_out
    )
    mine = added(mine, core_swap(theirs))
    mine, routes, route_weights = lax.optimization_barrier((mine, routes, route_weights))
    matrices = tables(routes, route_weights, core, chip, share_rows, experts, capacity)
    *others, table, pick, place = lax.optimization_barrier((*from_chips(mine), *matrices))
    mixout = chip_sum(mine, *others)
    resid = lax.dynamic_slice_in_dim(tokens, core * half, half, 0).astype(F32) + mixout
    rows = (resid * mean_scale(resid) * ffn_gain).astype(BF16)
    packet = build(table, rows, core_swap(rows)).reshape(groups, capacity, width)
    packet = lax.all_to_all(packet, "ep", split_axis=0, concat_axis=0, tiled=True)
    packet = packet.reshape(groups * capacity, width)
    other = core_swap(packet)
    dense = dense_share(packet, dense_gate.T, dense_up.T, dense_down)
    packet = ffn(
        packet, other, dense, expert_gate[0].T, expert_up[0].T, expert_down[0]
    ).reshape(groups, capacity, width + wide)
    packet = lax.all_to_all(packet, "ep", split_axis=0, concat_axis=0, tiled=True)
    mine, theirs = combine(pick, packet.reshape(groups * capacity, -1), dense_mix, place)
    mine = added(mine, core_swap(theirs))
    mixed = (resid + chip_sum(mine, *from_chips(mine))).astype(BF16)
    other = core_swap(mixed)
    first = jnp.where(core == 0, mixed, other)
    second = jnp.where(core == 0, other, mixed)
    return (jnp.concatenate([first, second], axis=0), new_state)


def solution(mesh):
    in_specs = (
        P("ep", None),
        P("ep", "tp", None, None),
        P(),
        P(None, "tp"),
        P(None, "tp"),
        P(None, "tp"),
        P(None, "tp"),
        P("tp"),
        P(),
        P("tp", None),
        P(),
        P("ep", None),
        P("ep", None),
        P("ep", None, "tp"),
        P("ep", None, "tp"),
        P("ep", "tp", None),
        P(None, "ep"),
        P(None, "ep"),
        P("ep", None),
        P(),
    )
    out_specs = (P("ep", None), P("ep", "tp", None, None))
    return jax.shard_map(local, mesh=mesh, in_specs=in_specs, out_specs=out_specs, check_vma=False)
```

```python
import jax
import jax.numpy as jnp
from jax import lax
from jax.experimental import pallas as pl
from jax.experimental.pallas import tpu as pltpu
from jax.sharding import PartitionSpec as P

EPS = 1e-06
F32 = jnp.float32
BF16 = jnp.bfloat16
HBM = pl.BlockSpec(memory_space=pltpu.HBM)
VMEM = pl.BlockSpec(memory_space=pltpu.VMEM)


CHUNKS = 4


def dot(a, b):
    return jnp.dot(a, b, preferred_element_type=F32)


def dot_t(a, b):
    return lax.dot_general(a, b, (((1,), (1,)), ((), ())), preferred_element_type=F32)


def mean_scale(x):
    return lax.rsqrt(jnp.mean(x * x, axis=-1, keepdims=True) + EPS)


def this_core():
    return lax.rem(lax.axis_index("tp"), 2)


def by_core(x, core):
    half = x.shape[1] // 2
    low, high = x[:, :half], x[:, half:]
    return jnp.where(core == 0, low, high), jnp.where(core == 0, high, low)


def sigmoid(x):
    return 1.0 / (1.0 + jnp.exp(-x))


def mixer_kernel(
    tokens_in,
    gain_in,
    floor_in,
    head_gain_in,
    state,
    w_query,
    w_forget,
    w_input,
    w_outgate,
    w_out,
    new_state,
    mine,
    theirs,
    tokens,
    gain,
    floor,
    head_gain,
    w_buf,
    wo_buf,
    held,
    spread,
    columns,
    values,
    read,
    small_sem,
    w_sem,
    wo_sem,
    in_sem,
    out_sem,
):
    seqs = tokens.shape[0]
    heads, size = held.shape[1:3]
    step = seqs // CHUNKS
    core = this_core()
    small = [
        pltpu.make_async_copy(a, b, small_sem.at[i])
        for i, (a, b) in enumerate(
            ((tokens_in, tokens), (gain_in, gain), (floor_in, floor), (head_gain_in, head_gain))
        )
    ]
    for load in small:
        load.start()
    loads = [
        pltpu.make_async_copy(w, w_buf.at[i], w_sem.at[i])
        for i, w in enumerate((w_forget, w_query, w_input, w_outgate))
    ]
    for load in loads[:3]:
        load.start()

    def fetch(j):
        rows = pl.ds(j * step, step)
        return pltpu.make_async_copy(state.at[rows], held.at[rows], in_sem.at[j])

    def flush_half(j, part):
        rows = pl.ds(j * step + part * (step // 2), step // 2)
        return pltpu.make_async_copy(held.at[rows], new_state.at[rows], out_sem.at[2 * j + part])

    for load in small[:2]:
        load.wait()
    x = tokens[...].astype(F32)
    normed = (x * mean_scale(x) * gain[...]).astype(BF16)
    for j in range(2):
        fetch(j).start()
    for load in small[2:]:
        load.wait()
    base = floor[...]
    row = lax.broadcasted_iota(jnp.int32, spread.shape[1:], 0)
    lane = lax.broadcasted_iota(jnp.int32, spread.shape[1:], 1)
    source = jnp.where(row < 3 * seqs, row % seqs - lane // size, -1)
    for p in range(spread.shape[0]):
        spread[p] = jnp.where(source == 2 * p, 1.0, 0.0).astype(BF16)
    loads[0].wait()
    for j in range(2, CHUNKS):
        fetch(j).start()
    keep = base + (1.0 - base) * sigmoid(dot(normed, w_buf[0]))
    loads[1].wait()
    loads[3].start()
    load_out = pltpu.make_async_copy(w_out, wo_buf, wo_sem)
    load_out.start()
    zq = dot(normed, w_buf[1])
    both = jnp.concatenate([keep, zq * sigmoid(zq)], axis=1)
    parts = []
    for _ in range(3):
        parts.append(both.astype(BF16).astype(F32))
        both = both - parts[-1]
    parts.append(jnp.zeros((size - 3 * seqs, both.shape[1]), F32))
    columns[...] = jnp.concatenate(parts, axis=0).T.astype(BF16)
    loads[2].wait()
    values[...] = dot(normed, w_buf[2])

    def body(j, carry):
        fetch(j).wait()
        rows = pl.ds(pl.multiple_of(j * step, step), step)
        block = values[rows, :]
        reads = [[None] * heads for _ in range(step)]
        for p in range(step // 2):
            one = spread[j * (step // 2) + p]
            for h in range(heads):
                at = h * size
                keeps = dot(columns[at : at + size, :], one)
                queries = dot(columns[(heads + h) * size : (heads + h + 1) * size, :], one)
                for i in range(2):
                    t = 2 * p + i
                    v = block[t : t + 1, at : at + size]
                    lanes = slice(i * size, (i + 1) * size)
                    new = v + keeps[:, lanes] * (held[j * step + t, h] - v)
                    held[j * step + t, h] = new
                    reads[t][h] = jnp.sum(queries[:, lanes] * new, axis=0, keepdims=True)
            if p % (step // 4) == step // 4 - 1:
                flush_half(j, p // (step // 4)).start()
        read[rows, :] = jnp.concatenate([jnp.concatenate(r, axis=1) for r in reads], axis=0)
        return carry

    lax.fori_loop(0, CHUNKS, body, 0)
    loads[3].wait()
    zg = dot(normed, w_buf[3])
    gate = zg * sigmoid(zg)
    outs = []
    for h in range(heads):
        lanes = slice(h * size, (h + 1) * size)
        r = read[:, lanes]
        outs.append(r * mean_scale(r) * head_gain[...] * gate[:, lanes])
    headout = jnp.concatenate(outs, axis=1).astype(BF16)
    load_out.wait()
    block = dot(headout, wo_buf[...])
    mine[...], theirs[...] = by_core(block.astype(BF16), core)
    for j in range(CHUNKS):
        for part in range(2):
            flush_half(j, part).wait()


def mixer(tokens, state, norm_gain, w_query, w_forget, w_input, w_outgate, floor, head_gain, w_out):
    seqs, width = tokens.shape
    channels = w_query.shape[1]
    half = jax.ShapeDtypeStruct((seqs, width // 2), BF16)
    size = state.shape[3]
    return pl.pallas_call(
        mixer_kernel,
        out_shape=(jax.ShapeDtypeStruct(state.shape, state.dtype), half, half),
        in_specs=[HBM] * 10,
        out_specs=(HBM, VMEM, VMEM),
        scratch_shapes=[
            pltpu.VMEM((seqs, width), BF16),
            pltpu.VMEM((1, width), F32),
            pltpu.VMEM((1, channels), F32),
            pltpu.VMEM((1, state.shape[3]), F32),
            pltpu.VMEM((4, width, channels), BF16),
            pltpu.VMEM((channels, width), BF16),
            pltpu.VMEM(state.shape, F32),
            pltpu.VMEM((seqs // 2, size, 2 * size), BF16),
            pltpu.VMEM((2 * channels, size), BF16),
            pltpu.VMEM((seqs, channels), F32),
            pltpu.VMEM((seqs, channels), F32),
            pltpu.SemaphoreType.DMA((4,)),
            pltpu.SemaphoreType.DMA((4,)),
            pltpu.SemaphoreType.DMA,
            pltpu.SemaphoreType.DMA((CHUNKS,)),
            pltpu.SemaphoreType.DMA((2 * CHUNKS,)),
        ],
        compiler_params=pltpu.CompilerParams(vmem_limit_bytes=20 << 20),
        name="mixer",
    )(
        *(
            pltpu.with_memory_space_constraint(x, pltpu.HBM)
            for x in (
                tokens,
                norm_gain.reshape(1, width),
                floor.reshape(1, channels),
                head_gain.reshape(1, -1),
                state,
                w_query,
                w_forget,
                w_input,
                w_outgate,
                w_out,
            )
        )
    )


def build_kernel(table, tokens, gain, resid, other, packet):
    core = this_core()
    there = by_core(tokens[...].astype(F32), core)[1] + other[...].astype(F32)
    here = resid[...]
    x = jnp.concatenate(
        [jnp.where(core == 0, here, there), jnp.where(core == 0, there, here)], axis=1
    )
    rows = (x * mean_scale(x) * gain[...]).astype(BF16)
    packet[...] = dot(table[...], rows).astype(BF16)


def build(table, tokens, gain, resid, other):
    width = tokens.shape[1]
    return pl.pallas_call(
        build_kernel,
        out_shape=jax.ShapeDtypeStruct((table.shape[0], width), BF16),
        in_specs=[VMEM] * 5,
        out_specs=VMEM,
        compiler_params=pltpu.CompilerParams(vmem_limit_bytes=8 << 20),
        cost_estimate=pl.CostEstimate(flops=10**10, bytes_accessed=10**8, transcendentals=0),
        name="build",
    )(table, tokens, gain.reshape(1, width), resid, other)


def own_slots(shape, group, core):
    at = lax.broadcasted_iota(jnp.int32, shape, 0)
    return (at % group) // (group // 2) == core


def dense_kernel(packet, gate_w, up_w, down_w, mine, theirs):
    share = packet[...]
    gate = dot_t(share, gate_w[...])
    upper = dot_t(share, up_w[...])
    hidden = (gate * sigmoid(gate) * upper).astype(BF16)
    result = dot(hidden, down_w[...]).astype(BF16)
    mine[...], theirs[...] = by_core(result, this_core())


def dense_share(packet, gate_w, up_w, down_w):
    rows, width = packet.shape
    half = jax.ShapeDtypeStruct((rows, width // 2), BF16)
    return pl.pallas_call(
        dense_kernel,
        out_shape=(half, half),
        in_specs=[VMEM] * 4,
        out_specs=(VMEM, VMEM),
        compiler_params=pltpu.CompilerParams(vmem_limit_bytes=16 << 20),
        name="dense",
    )(packet, gate_w, up_w, down_w)


def ffn_kernel(packet, other, e_gate, e_up, e_down, mine, theirs):
    core = this_core()
    own = own_slots(packet.shape, 8, core)
    rows = jnp.where(own, packet[...].astype(F32), other[...].astype(F32)).astype(BF16)
    gate = dot_t(rows, e_gate[...])
    upper = dot_t(rows, e_up[...])
    hidden = (gate * sigmoid(gate) * upper).astype(BF16)
    mine[...], theirs[...] = by_core(dot(hidden, e_down[...]).astype(BF16), core)


def ffn(packet, other, e_gate, e_up, e_down):
    rows, width = packet.shape
    half = jax.ShapeDtypeStruct((rows, width // 2), BF16)
    return pl.pallas_call(
        ffn_kernel,
        out_shape=(half, half),
        in_specs=[VMEM] * 5,
        out_specs=(VMEM, VMEM),
        compiler_params=pltpu.CompilerParams(vmem_limit_bytes=24 << 20),
        name="ffn",
    )(packet, other, e_gate, e_up, e_down)


def merge_kernel(part, other_part, share, other_share, packet):
    half = part.shape[1]
    packet[:, :half] = (part[...].astype(F32) + other_part[...].astype(F32)).astype(BF16)
    own = own_slots(part.shape, 8, this_core())
    both = jnp.where(own, other_share[...].astype(F32), share[...].astype(F32))
    packet[:, half:] = both.astype(BF16)


def merge(part, other_part, share, other_share):
    rows, half = part.shape
    return pl.pallas_call(
        merge_kernel,
        out_shape=jax.ShapeDtypeStruct((rows, 2 * half), BF16),
        in_specs=[VMEM] * 4,
        out_specs=VMEM,
        compiler_params=pltpu.CompilerParams(vmem_limit_bytes=8 << 20),
        name="merge",
    )(part, other_part, share, other_share)


def combine_kernel(pick, packet, mix, place, out):
    seqs, half = out.shape
    group = 8
    moe = dot(pick[...], packet[:, :half])
    total = moe[:seqs] + moe[seqs:]
    parts = packet[:, half:].astype(F32)
    dense = jnp.sum(parts.reshape(-1, group, half), axis=0)
    dense = sigmoid(by_core(mix[...], this_core())[0]) * dense
    where = place[...]
    for r in range(group):
        total = total + where[:, r : r + 1] * dense[r : r + 1]
    out[...] = total.astype(BF16)


def combine(pick, packet, mix, place):
    width = mix.shape[0]
    return pl.pallas_call(
        combine_kernel,
        out_shape=jax.ShapeDtypeStruct((pick.shape[0] // 2, width // 2), BF16),
        in_specs=[VMEM] * 4,
        out_specs=VMEM,
        compiler_params=pltpu.CompilerParams(vmem_limit_bytes=8 << 20),
        name="combine",
    )(pick, packet, mix.reshape(1, width), place)


def routing(local_routes, experts, capacity):
    flat = local_routes.reshape(-1)
    onehot = (flat[:, None] == jnp.arange(experts, dtype=jnp.int32)[None, :]).astype(jnp.int32)
    before = jnp.cumsum(onehot, axis=0) - onehot
    slot = jnp.sum(before * onehot, axis=1)
    where = (flat * capacity + slot).reshape(local_routes.shape)
    return where[:, :, None] == jnp.arange(experts * capacity, dtype=jnp.int32)[None, None, :]


def core_swap(x):
    return lax.ppermute(x, "tp", [(t, t ^ 1) for t in range(8)])


def added(mine, other):
    return (mine.astype(F32) + other.astype(F32)).astype(BF16)


def from_chips(mine):
    return [lax.ppermute(mine, "tp", [(t, t ^ d) for t in range(8)]) for d in (4, 2, 6)]


def chip_sum(mine, far, near, across):
    return (mine.astype(F32) + near.astype(F32)) + (far.astype(F32) + across.astype(F32))


def tables(routes, route_weights, core, chip, share_rows, experts, capacity):
    seqs = routes.shape[0]
    half = seqs // 2
    hits = routing(routes, experts, capacity)
    slots = jnp.any(hits, axis=1).T
    pick = jnp.sum(hits * route_weights[:, :, None], axis=1)
    high = pick.astype(BF16)
    low = (pick - high.astype(F32)).astype(BF16)
    pick = jnp.concatenate([high, low], axis=0)
    token = jnp.arange(seqs, dtype=jnp.int32)
    row = jnp.arange(slots.shape[0], dtype=jnp.int32)[:, None]
    share = core * half + chip * share_rows + row % share_rows == token[None, :]
    own = row % capacity // share_rows == core
    table = jnp.where(own, slots, share).astype(BF16)
    row = jnp.arange(capacity, dtype=jnp.int32)[None, :]
    place = (1 - row // share_rows) * half + chip * share_rows + row % share_rows
    return table, pick, (place == token[:, None]).astype(F32)


def local(
    tokens,
    state,
    norm_gain,
    w_query,
    w_forget,
    w_input,
    w_outgate,
    forget_floor,
    head_gain,
    w_out,
    ffn_gain,
    routes,
    route_weights,
    expert_gate,
    expert_up,
    expert_down,
    dense_gate,
    dense_up,
    dense_down,
    dense_mix,
):
    seqs, width = tokens.shape
    tp = lax.axis_index("tp")
    core, chip = tp % 2, tp // 2
    half = width // 2
    groups = lax.axis_size("ep")
    experts = groups * expert_gate.shape[0]
    top = routes.shape[1]
    capacity = 2 * seqs * top // experts
    share_rows = seqs // lax.axis_size("tp")

    new_state, mine, theirs = mixer(
        tokens, state, norm_gain, w_query, w_forget, w_input, w_outgate, forget_floor, head_gain, w_out
    )
    mine = added(mine, core_swap(theirs))
    mine, routes, route_weights = lax.optimization_barrier((mine, routes, route_weights))
    matrices = tables(routes, route_weights, core, chip, share_rows, experts, capacity)
    *others, table, pick, place = lax.optimization_barrier((*from_chips(mine), *matrices))
    mixout = chip_sum(mine, *others)
    resid = lax.dynamic_slice_in_dim(tokens, core * half, half, 1).astype(F32) + mixout
    packet = build(table, tokens, ffn_gain, resid, core_swap(mixout.astype(BF16)))
    packet = packet.reshape(groups, capacity, width)
    packet = lax.all_to_all(packet, "ep", split_axis=0, concat_axis=0, tiled=True)
    packet = packet.reshape(groups * capacity, width)
    other = core_swap(packet)
    share, theirs = dense_share(packet, dense_gate.T, dense_up.T, dense_down)
    other_share = core_swap(theirs)
    part, theirs = ffn(packet, other, expert_gate[0].T, expert_up[0].T, expert_down[0])
    packet = merge(part, core_swap(theirs), share, other_share)
    packet = packet.reshape(groups, capacity, width)
    packet = lax.all_to_all(packet, "ep", split_axis=0, concat_axis=0, tiled=True)
    mine = combine(pick, packet.reshape(groups * capacity, width), dense_mix, place)
    mixed = (resid + chip_sum(mine, *from_chips(mine))).astype(BF16)
    other = core_swap(mixed)
    first = jnp.where(core == 0, mixed, other)
    second = jnp.where(core == 0, other, mixed)
    return (jnp.concatenate([first, second], axis=1), new_state)


def solution(mesh):
    in_specs = (
        P("ep", None),
        P("ep", "tp", None, None),
        P(),
        P(None, "tp"),
        P(None, "tp"),
        P(None, "tp"),
        P(None, "tp"),
        P("tp"),
        P(),
        P("tp", None),
        P(),
        P("ep", None),
        P("ep", None),
        P("ep", None, "tp"),
        P("ep", None, "tp"),
        P("ep", "tp", None),
        P(None, "ep"),
        P(None, "ep"),
        P("ep", None),
        P(),
    )
    out_specs = (P("ep", None), P("ep", "tp", None, None))
    return jax.shard_map(local, mesh=mesh, in_specs=in_specs, out_specs=out_specs, check_vma=False)
```

```python
import jax
import jax.numpy as jnp
from jax import lax
from jax.experimental import pallas as pl
from jax.experimental.pallas import tpu as pltpu
from jax.sharding import PartitionSpec as P

EPS = 1e-06
F32 = jnp.float32
BF16 = jnp.bfloat16
HBM = pl.BlockSpec(memory_space=pltpu.HBM)
VMEM = pl.BlockSpec(memory_space=pltpu.VMEM)


CHUNKS = 4


def dot(a, b):
    return jnp.dot(a, b, preferred_element_type=F32)


def dot_t(a, b):
    return lax.dot_general(a, b, (((1,), (1,)), ((), ())), preferred_element_type=F32)


def mean_scale(x):
    return lax.rsqrt(jnp.mean(x * x, axis=-1, keepdims=True) + EPS)


def this_core():
    return lax.rem(lax.axis_index("tp"), 2)


def by_core(x, core):
    half = x.shape[1] // 2
    low, high = x[:, :half], x[:, half:]
    return jnp.where(core == 0, low, high), jnp.where(core == 0, high, low)


def sigmoid(x):
    return 1.0 / (1.0 + jnp.exp(-x))


def mixer_kernel(
    tokens_in,
    gain_in,
    floor_in,
    head_gain_in,
    state,
    w_query,
    w_forget,
    w_input,
    w_outgate,
    w_out,
    new_state,
    mine,
    theirs,
    tokens,
    gain,
    floor,
    head_gain,
    w_buf,
    wo_buf,
    held,
    spread,
    columns,
    values,
    read,
    small_sem,
    w_sem,
    wo_sem,
    in_sem,
    out_sem,
):
    seqs = tokens.shape[0]
    heads, size = held.shape[1:3]
    step = seqs // CHUNKS
    core = this_core()
    small = [
        pltpu.make_async_copy(a, b, small_sem.at[i])
        for i, (a, b) in enumerate(
            ((tokens_in, tokens), (gain_in, gain), (floor_in, floor), (head_gain_in, head_gain))
        )
    ]
    for load in small:
        load.start()
    loads = [
        pltpu.make_async_copy(w, w_buf.at[i], w_sem.at[i])
        for i, w in enumerate((w_forget, w_query, w_input, w_outgate))
    ]
    for load in loads[:3]:
        load.start()

    def fetch(j):
        rows = pl.ds(j * step, step)
        return pltpu.make_async_copy(state.at[rows], held.at[rows], in_sem.at[j])

    def flush_half(j, part):
        rows = pl.ds(j * step + part * (step // 2), step // 2)
        return pltpu.make_async_copy(held.at[rows], new_state.at[rows], out_sem.at[2 * j + part])

    for load in small[:2]:
        load.wait()
    x = tokens[...].astype(F32)
    normed = (x * mean_scale(x) * gain[...]).astype(BF16)
    for j in range(2):
        fetch(j).start()
    for load in small[2:]:
        load.wait()
    base = floor[...]
    row = lax.broadcasted_iota(jnp.int32, spread.shape[1:], 0)
    lane = lax.broadcasted_iota(jnp.int32, spread.shape[1:], 1)
    source = jnp.where(row < 3 * seqs, row % seqs - lane // size, -1)
    for p in range(spread.shape[0]):
        spread[p] = jnp.where(source == 2 * p, 1.0, 0.0).astype(BF16)
    loads[0].wait()
    for j in range(2, CHUNKS):
        fetch(j).start()
    keep = base + (1.0 - base) * sigmoid(dot(normed, w_buf[0]))
    loads[1].wait()
    loads[3].start()
    load_out = pltpu.make_async_copy(w_out, wo_buf, wo_sem)
    load_out.start()
    zq = dot(normed, w_buf[1])
    both = jnp.concatenate([keep, zq * sigmoid(zq)], axis=1)
    parts = []
    for _ in range(3):
        parts.append(both.astype(BF16).astype(F32))
        both = both - parts[-1]
    parts.append(jnp.zeros((size - 3 * seqs, both.shape[1]), F32))
    columns[...] = jnp.concatenate(parts, axis=0).T.astype(BF16)
    loads[2].wait()
    values[...] = dot(normed, w_buf[2])

    def body(j, carry):
        fetch(j).wait()
        rows = pl.ds(pl.multiple_of(j * step, step), step)
        block = values[rows, :]
        reads = [[None] * heads for _ in range(step)]
        for p in range(step // 2):
            one = spread[j * (step // 2) + p]
            for h in range(heads):
                at = h * size
                keeps = dot(columns[at : at + size, :], one)
                queries = dot(columns[(heads + h) * size : (heads + h + 1) * size, :], one)
                for i in range(2):
                    t = 2 * p + i
                    v = block[t : t + 1, at : at + size]
                    lanes = slice(i * size, (i + 1) * size)
                    new = v + keeps[:, lanes] * (held[j * step + t, h] - v)
                    held[j * step + t, h] = new
                    reads[t][h] = jnp.sum(queries[:, lanes] * new, axis=0, keepdims=True)
            if p % (step // 4) == step // 4 - 1:
                flush_half(j, p // (step // 4)).start()
        read[rows, :] = jnp.concatenate([jnp.concatenate(r, axis=1) for r in reads], axis=0)
        return carry

    lax.fori_loop(0, CHUNKS, body, 0)
    loads[3].wait()
    zg = dot(normed, w_buf[3])
    gate = zg * sigmoid(zg)
    outs = []
    for h in range(heads):
        lanes = slice(h * size, (h + 1) * size)
        r = read[:, lanes]
        outs.append(r * mean_scale(r) * head_gain[...] * gate[:, lanes])
    headout = jnp.concatenate(outs, axis=1).astype(BF16)
    load_out.wait()
    block = dot(headout, wo_buf[...])
    mine[...], theirs[...] = by_core(block.astype(BF16), core)
    for j in range(CHUNKS):
        for part in range(2):
            flush_half(j, part).wait()


def mixer(tokens, state, norm_gain, w_query, w_forget, w_input, w_outgate, floor, head_gain, w_out):
    seqs, width = tokens.shape
    channels = w_query.shape[1]
    half = jax.ShapeDtypeStruct((seqs, width // 2), BF16)
    size = state.shape[3]
    return pl.pallas_call(
        mixer_kernel,
        out_shape=(jax.ShapeDtypeStruct(state.shape, state.dtype), half, half),
        in_specs=[HBM] * 10,
        out_specs=(HBM, VMEM, VMEM),
        scratch_shapes=[
            pltpu.VMEM((seqs, width), BF16),
            pltpu.VMEM((1, width), F32),
            pltpu.VMEM((1, channels), F32),
            pltpu.VMEM((1, state.shape[3]), F32),
            pltpu.VMEM((4, width, channels), BF16),
            pltpu.VMEM((channels, width), BF16),
            pltpu.VMEM(state.shape, F32),
            pltpu.VMEM((seqs // 2, size, 2 * size), BF16),
            pltpu.VMEM((2 * channels, size), BF16),
            pltpu.VMEM((seqs, channels), F32),
            pltpu.VMEM((seqs, channels), F32),
            pltpu.SemaphoreType.DMA((4,)),
            pltpu.SemaphoreType.DMA((4,)),
            pltpu.SemaphoreType.DMA,
            pltpu.SemaphoreType.DMA((CHUNKS,)),
            pltpu.SemaphoreType.DMA((2 * CHUNKS,)),
        ],
        compiler_params=pltpu.CompilerParams(vmem_limit_bytes=20 << 20),
        name="mixer",
    )(
        *(
            pltpu.with_memory_space_constraint(x, pltpu.HBM)
            for x in (
                tokens,
                norm_gain.reshape(1, width),
                floor.reshape(1, channels),
                head_gain.reshape(1, -1),
                state,
                w_query,
                w_forget,
                w_input,
                w_outgate,
                w_out,
            )
        )
    )


def build_kernel(table, resid, packet):
    half = resid.shape[1]
    rows = dot(table[...], resid[...].astype(BF16)).astype(BF16)
    packet[:, :half] = rows[: packet.shape[0]]
    packet[:, half:] = rows[packet.shape[0] :]


def build(table, resid):
    rows, half = table.shape[0] // 2, resid.shape[1]
    return pl.pallas_call(
        build_kernel,
        out_shape=jax.ShapeDtypeStruct((rows, 2 * half), BF16),
        in_specs=[VMEM] * 2,
        out_specs=VMEM,
        compiler_params=pltpu.CompilerParams(vmem_limit_bytes=8 << 20),
        cost_estimate=pl.CostEstimate(flops=10**10, bytes_accessed=10**8, transcendentals=0),
        name="build",
    )(table, resid)


def partial_products(packet, gain, core, weights):
    half = packet.shape[1] // 2
    scale = jnp.where(core == 0, gain[:, :half], gain[:, half:])
    columns = pl.ds(pl.multiple_of(core * half, half), half)
    routed = (packet[:, :half].astype(F32) * scale).astype(BF16)
    share = (packet[:, half:].astype(F32) * scale).astype(BF16)
    rows = (routed, routed, share, share)
    return [dot_t(x, w[:, columns]) for x, w in zip(rows, weights)]


def front_kernel(packet, gain, e_gate, e_up, d_gate, d_up, *outs):
    products = partial_products(packet, gain, this_core(), (e_gate, e_up, d_gate, d_up))
    for out, product in zip(outs, products):
        out[...] = product


def front(packet, gain, *weights):
    rows, width = packet.shape
    return pl.pallas_call(
        front_kernel,
        out_shape=[jax.ShapeDtypeStruct((rows, w.shape[0]), F32) for w in weights],
        in_specs=[VMEM] * 6,
        out_specs=[VMEM] * 4,
        compiler_params=pltpu.CompilerParams(vmem_limit_bytes=24 << 20),
        name="front",
    )(packet, gain.reshape(1, width), *weights)


def squares(packet, at):
    x = packet[:, at].astype(F32)
    return jnp.sum(x * x, axis=-1, keepdims=True)


def back_kernel(
    packet,
    other,
    gain,
    gate_e,
    up_e,
    gate_d,
    up_d,
    e_gate,
    e_up,
    d_gate,
    d_up,
    e_down,
    d_down,
    mine,
    theirs,
    share,
):
    width = packet.shape[1]
    half = width // 2
    core = this_core()
    rest = partial_products(other, gain, 1 - core, (e_gate, e_up, d_gate, d_up))
    at = slice(0, half)
    scale = lax.rsqrt((squares(packet, at) + squares(other, at)) / width + EPS)
    gate = (gate_e[...] + rest[0]) * scale
    upper = (up_e[...] + rest[1]) * scale
    hidden = (gate * sigmoid(gate) * upper).astype(BF16)
    mine[...], theirs[...] = by_core(dot(hidden, e_down[...]).astype(BF16), core)
    at = slice(half, width)
    scale = lax.rsqrt((squares(packet, at) + squares(other, at)) / width + EPS)
    gate = (gate_d[...] + rest[2]) * scale
    upper = (up_d[...] + rest[3]) * scale
    hidden = (gate * sigmoid(gate) * upper).astype(BF16)
    columns = pl.ds(pl.multiple_of(core * half, half), half)
    share[...] = dot(hidden, d_down[:, columns]).astype(BF16)


def back(packet, other, gain, partial, *weights):
    rows, width = packet.shape
    half = jax.ShapeDtypeStruct((rows, width // 2), BF16)
    return pl.pallas_call(
        back_kernel,
        out_shape=(half, half, half),
        in_specs=[VMEM] * 13,
        out_specs=(VMEM, VMEM, VMEM),
        compiler_params=pltpu.CompilerParams(vmem_limit_bytes=32 << 20),
        name="back",
    )(packet, other, gain.reshape(1, width), *partial, *weights)


def merge_kernel(part, other_part, share, packet):
    half = part.shape[1]
    packet[:, :half] = (part[...].astype(F32) + other_part[...].astype(F32)).astype(BF16)
    packet[:, half:] = share[...]


def merge(part, other_part, share):
    rows, half = part.shape
    return pl.pallas_call(
        merge_kernel,
        out_shape=jax.ShapeDtypeStruct((rows, 2 * half), BF16),
        in_specs=[VMEM] * 3,
        out_specs=VMEM,
        compiler_params=pltpu.CompilerParams(vmem_limit_bytes=8 << 20),
        name="merge",
    )(part, other_part, share)


def combine_kernel(pick, packet, mix, place, out):
    seqs, half = out.shape
    group = 8
    moe = dot(pick[...], packet[:, :half])
    total = moe[:seqs] + moe[seqs:]
    parts = packet[:, half:].astype(F32)
    dense = jnp.sum(parts.reshape(-1, group, half), axis=0)
    dense = sigmoid(by_core(mix[...], this_core())[0]) * dense
    where = place[...]
    for r in range(group):
        total = total + where[:, r : r + 1] * dense[r : r + 1]
    out[...] = total.astype(BF16)


def combine(pick, packet, mix, place):
    width = mix.shape[0]
    return pl.pallas_call(
        combine_kernel,
        out_shape=jax.ShapeDtypeStruct((pick.shape[0] // 2, width // 2), BF16),
        in_specs=[VMEM] * 4,
        out_specs=VMEM,
        compiler_params=pltpu.CompilerParams(vmem_limit_bytes=8 << 20),
        name="combine",
    )(pick, packet, mix.reshape(1, width), place)


def routing(local_routes, experts, capacity):
    flat = local_routes.reshape(-1)
    onehot = (flat[:, None] == jnp.arange(experts, dtype=jnp.int32)[None, :]).astype(jnp.int32)
    before = jnp.cumsum(onehot, axis=0) - onehot
    slot = jnp.sum(before * onehot, axis=1)
    where = (flat * capacity + slot).reshape(local_routes.shape)
    return where[:, :, None] == jnp.arange(experts * capacity, dtype=jnp.int32)[None, None, :]


def core_swap(x):
    return lax.ppermute(x, "tp", [(t, t ^ 1) for t in range(8)])


def added(mine, other):
    return (mine.astype(F32) + other.astype(F32)).astype(BF16)


def from_chips(mine):
    return [lax.ppermute(mine, "tp", [(t, t ^ d) for t in range(8)]) for d in (4, 2, 6)]


def chip_sum(mine, far, near, across):
    return (mine.astype(F32) + near.astype(F32)) + (far.astype(F32) + across.astype(F32))


def tables(routes, route_weights, chip, share_rows, experts, capacity):
    seqs = routes.shape[0]
    hits = routing(routes, experts, capacity)
    slots = jnp.any(hits, axis=1)
    pick = jnp.sum(hits * route_weights[:, :, None], axis=1)
    high = pick.astype(BF16)
    low = (pick - high.astype(F32)).astype(BF16)
    pick = jnp.concatenate([high, low], axis=0)
    token = jnp.arange(seqs, dtype=jnp.int32)[:, None]
    row = jnp.arange(slots.shape[1], dtype=jnp.int32)[None, :]
    place = chip * share_rows + row % share_rows == token
    table = jnp.concatenate([slots, place], axis=1).astype(BF16).T
    return table, pick, place[:, :share_rows].astype(F32)


def local(
    tokens,
    state,
    norm_gain,
    w_query,
    w_forget,
    w_input,
    w_outgate,
    forget_floor,
    head_gain,
    w_out,
    ffn_gain,
    routes,
    route_weights,
    expert_gate,
    expert_up,
    expert_down,
    dense_gate,
    dense_up,
    dense_down,
    dense_mix,
):
    seqs, width = tokens.shape
    tp = lax.axis_index("tp")
    core, chip = tp % 2, tp // 2
    half = width // 2
    groups = lax.axis_size("ep")
    experts = groups * expert_gate.shape[0]
    top = routes.shape[1]
    capacity = 2 * seqs * top // experts
    share_rows = 2 * seqs // lax.axis_size("tp")

    new_state, mine, theirs = mixer(
        tokens, state, norm_gain, w_query, w_forget, w_input, w_outgate, forget_floor, head_gain, w_out
    )
    mine = added(mine, core_swap(theirs))
    mine, routes, route_weights = lax.optimization_barrier((mine, routes, route_weights))
    matrices = tables(routes, route_weights, chip, share_rows, experts, capacity)
    *others, table, pick, place = lax.optimization_barrier((*from_chips(mine), *matrices))
    mixout = chip_sum(mine, *others)
    resid = lax.dynamic_slice_in_dim(tokens, core * half, half, 1).astype(F32) + mixout
    packet = build(table, resid).reshape(groups, capacity, width)
    packet = lax.all_to_all(packet, "ep", split_axis=0, concat_axis=0, tiled=True)
    packet = packet.reshape(groups * capacity, width)
    other = core_swap(packet)
    weights = (expert_gate[0].T, expert_up[0].T, dense_gate.T, dense_up.T)
    partial = front(packet, ffn_gain, *weights)
    part, theirs, share = back(
        packet, other, ffn_gain, partial, *weights, expert_down[0], dense_down
    )
    packet = merge(part, core_swap(theirs), share).reshape(groups, capacity, width)
    packet = lax.all_to_all(packet, "ep", split_axis=0, concat_axis=0, tiled=True)
    mine = combine(pick, packet.reshape(groups * capacity, width), dense_mix, place)
    mixed = (resid + chip_sum(mine, *from_chips(mine))).astype(BF16)
    other = core_swap(mixed)
    first = jnp.where(core == 0, mixed, other)
    second = jnp.where(core == 0, other, mixed)
    return (jnp.concatenate([first, second], axis=1), new_state)


def solution(mesh):
    in_specs = (
        P("ep", None),
        P("ep", "tp", None, None),
        P(),
        P(None, "tp"),
        P(None, "tp"),
        P(None, "tp"),
        P(None, "tp"),
        P("tp"),
        P(),
        P("tp", None),
        P(),
        P("ep", None),
        P("ep", None),
        P("ep", None, "tp"),
        P("ep", None, "tp"),
        P("ep", "tp", None),
        P(None, "ep"),
        P(None, "ep"),
        P("ep", None),
        P(),
    )
    out_specs = (P("ep", None), P("ep", "tp", None, None))
    return jax.shard_map(local, mesh=mesh, in_specs=in_specs, out_specs=out_specs, check_vma=False)
```

```python
import jax
import jax.numpy as jnp
from jax import lax
from jax.experimental import pallas as pl
from jax.experimental.pallas import tpu as pltpu
from jax.sharding import PartitionSpec as P

EPS = 1e-06
F32 = jnp.float32
BF16 = jnp.bfloat16
HBM = pl.BlockSpec(memory_space=pltpu.HBM)
VMEM = pl.BlockSpec(memory_space=pltpu.VMEM)


CHUNKS = 4


def dot(a, b):
    return jnp.dot(a, b, preferred_element_type=F32)


def dot_t(a, b):
    return lax.dot_general(a, b, (((1,), (1,)), ((), ())), preferred_element_type=F32)


def mean_scale(x):
    return lax.rsqrt(jnp.mean(x * x, axis=-1, keepdims=True) + EPS)


def this_core():
    return lax.rem(lax.axis_index("tp"), 2)


def by_core(x, core):
    half = x.shape[1] // 2
    low, high = x[:, :half], x[:, half:]
    return jnp.where(core == 0, low, high), jnp.where(core == 0, high, low)


def sigmoid(x):
    return 1.0 / (1.0 + jnp.exp(-x))


def mixer_kernel(
    tokens_in,
    gain_in,
    floor_in,
    head_gain_in,
    state,
    w_query,
    w_forget,
    w_input,
    w_outgate,
    w_out,
    new_state,
    mine,
    theirs,
    tokens,
    gain,
    floor,
    head_gain,
    w_buf,
    wo_buf,
    held,
    spread,
    columns,
    values,
    read,
    small_sem,
    w_sem,
    wo_sem,
    in_sem,
    out_sem,
):
    seqs = tokens.shape[0]
    heads, size = held.shape[1:3]
    step = seqs // CHUNKS
    core = this_core()
    small = [
        pltpu.make_async_copy(a, b, small_sem.at[i])
        for i, (a, b) in enumerate(
            ((tokens_in, tokens), (gain_in, gain), (floor_in, floor), (head_gain_in, head_gain))
        )
    ]
    for load in small:
        load.start()
    loads = [
        pltpu.make_async_copy(w, w_buf.at[i], w_sem.at[i])
        for i, w in enumerate((w_forget, w_query, w_input, w_outgate))
    ]
    for load in loads[:3]:
        load.start()

    def fetch(j):
        rows = pl.ds(j * step, step)
        return pltpu.make_async_copy(state.at[rows], held.at[rows], in_sem.at[j])

    def flush_half(j, part):
        rows = pl.ds(j * step + part * (step // 2), step // 2)
        return pltpu.make_async_copy(held.at[rows], new_state.at[rows], out_sem.at[2 * j + part])

    for load in small[:2]:
        load.wait()
    x = tokens[...].astype(F32)
    normed = (x * mean_scale(x) * gain[...]).astype(BF16)
    for j in range(2):
        fetch(j).start()
    for load in small[2:]:
        load.wait()
    base = floor[...]
    row = lax.broadcasted_iota(jnp.int32, spread.shape[1:], 0)
    lane = lax.broadcasted_iota(jnp.int32, spread.shape[1:], 1)
    source = jnp.where(row < 3 * seqs, row % seqs - lane // size, -1)
    for p in range(spread.shape[0]):
        spread[p] = jnp.where(source == 2 * p, 1.0, 0.0).astype(BF16)
    loads[0].wait()
    for j in range(2, CHUNKS):
        fetch(j).start()
    keep = base + (1.0 - base) * sigmoid(dot(normed, w_buf[0]))
    loads[1].wait()
    loads[3].start()
    load_out = pltpu.make_async_copy(w_out, wo_buf, wo_sem)
    load_out.start()
    zq = dot(normed, w_buf[1])
    both = jnp.concatenate([keep, zq * sigmoid(zq)], axis=1)
    parts = []
    for _ in range(3):
        parts.append(both.astype(BF16).astype(F32))
        both = both - parts[-1]
    parts.append(jnp.zeros((size - 3 * seqs, both.shape[1]), F32))
    columns[...] = jnp.concatenate(parts, axis=0).T.astype(BF16)
    loads[2].wait()
    values[...] = dot(normed, w_buf[2])

    def body(j, carry):
        fetch(j).wait()
        rows = pl.ds(pl.multiple_of(j * step, step), step)
        block = values[rows, :]
        reads = [[None] * heads for _ in range(step)]
        for p in range(step // 2):
            one = spread[j * (step // 2) + p]
            for h in range(heads):
                at = h * size
                keeps = dot(columns[at : at + size, :], one)
                queries = dot(columns[(heads + h) * size : (heads + h + 1) * size, :], one)
                for i in range(2):
                    t = 2 * p + i
                    v = block[t : t + 1, at : at + size]
                    lanes = slice(i * size, (i + 1) * size)
                    new = v + keeps[:, lanes] * (held[j * step + t, h] - v)
                    held[j * step + t, h] = new
                    reads[t][h] = jnp.sum(queries[:, lanes] * new, axis=0, keepdims=True)
            if p % (step // 4) == step // 4 - 1:
                flush_half(j, p // (step // 4)).start()
        read[rows, :] = jnp.concatenate([jnp.concatenate(r, axis=1) for r in reads], axis=0)
        return carry

    lax.fori_loop(0, CHUNKS, body, 0)
    loads[3].wait()
    zg = dot(normed, w_buf[3])
    gate = zg * sigmoid(zg)
    outs = []
    for h in range(heads):
        lanes = slice(h * size, (h + 1) * size)
        r = read[:, lanes]
        outs.append(r * mean_scale(r) * head_gain[...] * gate[:, lanes])
    headout = jnp.concatenate(outs, axis=1).astype(BF16)
    load_out.wait()
    block = dot(headout, wo_buf[...])
    mine[...], theirs[...] = by_core(block.astype(BF16), core)
    for j in range(CHUNKS):
        for part in range(2):
            flush_half(j, part).wait()


def mixer(tokens, state, norm_gain, w_query, w_forget, w_input, w_outgate, floor, head_gain, w_out):
    seqs, width = tokens.shape
    channels = w_query.shape[1]
    half = jax.ShapeDtypeStruct((seqs, width // 2), BF16)
    size = state.shape[3]
    return pl.pallas_call(
        mixer_kernel,
        out_shape=(jax.ShapeDtypeStruct(state.shape, state.dtype), half, half),
        in_specs=[HBM] * 10,
        out_specs=(HBM, VMEM, VMEM),
        scratch_shapes=[
            pltpu.VMEM((seqs, width), BF16),
            pltpu.VMEM((1, width), F32),
            pltpu.VMEM((1, channels), F32),
            pltpu.VMEM((1, state.shape[3]), F32),
            pltpu.VMEM((4, width, channels), BF16),
            pltpu.VMEM((channels, width), BF16),
            pltpu.VMEM(state.shape, F32),
            pltpu.VMEM((seqs // 2, size, 2 * size), BF16),
            pltpu.VMEM((2 * channels, size), BF16),
            pltpu.VMEM((seqs, channels), F32),
            pltpu.VMEM((seqs, channels), F32),
            pltpu.SemaphoreType.DMA((4,)),
            pltpu.SemaphoreType.DMA((4,)),
            pltpu.SemaphoreType.DMA,
            pltpu.SemaphoreType.DMA((CHUNKS,)),
            pltpu.SemaphoreType.DMA((2 * CHUNKS,)),
        ],
        compiler_params=pltpu.CompilerParams(vmem_limit_bytes=20 << 20),
        name="mixer",
    )(
        *(
            pltpu.with_memory_space_constraint(x, pltpu.HBM)
            for x in (
                tokens,
                norm_gain.reshape(1, width),
                floor.reshape(1, channels),
                head_gain.reshape(1, -1),
                state,
                w_query,
                w_forget,
                w_input,
                w_outgate,
                w_out,
            )
        )
    )


def build_kernel(table, resid, packet):
    half = resid.shape[1]
    rows = dot(table[...], resid[...].astype(BF16)).astype(BF16)
    packet[:, :half] = rows[: packet.shape[0]]
    packet[:, half:] = rows[packet.shape[0] :]


def build(table, resid):
    rows, half = table.shape[0] // 2, resid.shape[1]
    return pl.pallas_call(
        build_kernel,
        out_shape=jax.ShapeDtypeStruct((rows, 2 * half), BF16),
        in_specs=[VMEM] * 2,
        out_specs=VMEM,
        compiler_params=pltpu.CompilerParams(vmem_limit_bytes=8 << 20),
        cost_estimate=pl.CostEstimate(flops=10**10, bytes_accessed=10**8, transcendentals=0),
        name="build",
    )(table, resid)


def columns_of(core, half):
    return pl.ds(pl.multiple_of(core * half, half), half)


def scaled(packet, at, gain, core):
    half = packet.shape[1] // 2
    factor = jnp.where(core == 0, gain[:, :half], gain[:, half:])
    return (packet[:, at].astype(F32) * factor).astype(BF16)


def row_scale(packet, other, at):
    mine, theirs = packet[:, at].astype(F32), other[:, at].astype(F32)
    total = jnp.sum(mine * mine, axis=-1, keepdims=True)
    total = total + jnp.sum(theirs * theirs, axis=-1, keepdims=True)
    return lax.rsqrt(total / packet.shape[1] + EPS)


def gated(gate, upper, scale):
    gate = gate * scale
    return (gate * sigmoid(gate) * (upper * scale)).astype(BF16)


def front_kernel(packet, gain, e_gate, e_up, d_gate, d_up, e_down, d_down, *outs):
    half = packet.shape[1] // 2
    core = this_core()
    columns = columns_of(core, half)
    routed = scaled(packet, slice(0, half), gain, core)
    share = scaled(packet, slice(half, 2 * half), gain, core)
    outs[0][...] = dot_t(routed, e_gate[:, columns])
    outs[1][...] = dot_t(routed, e_up[:, columns])
    outs[2][...] = dot_t(share, d_gate[:, columns])
    outs[3][...] = dot_t(share, d_up[:, columns])


def front(packet, gain, *weights):
    rows, width = packet.shape
    return pl.pallas_call(
        front_kernel,
        out_shape=[jax.ShapeDtypeStruct((rows, w.shape[0]), F32) for w in weights[:4]],
        in_specs=[VMEM] * 8,
        out_specs=[VMEM] * 4,
        compiler_params=pltpu.CompilerParams(vmem_limit_bytes=28 << 20),
        name="front",
    )(packet, gain, *weights)


def routed_kernel(packet, other, gain, gate, upper, e_gate, e_up, e_down, theirs, hidden):
    half = packet.shape[1] // 2
    there = 1 - this_core()
    columns = columns_of(there, half)
    at = slice(0, half)
    rows = scaled(other, at, gain, there)
    gate = gate[...] + dot_t(rows, e_gate[:, columns])
    upper = upper[...] + dot_t(rows, e_up[:, columns])
    value = gated(gate, upper, row_scale(packet, other, at))
    hidden[...] = value
    theirs[...] = dot(value, e_down[:, columns]).astype(BF16)


def routed(packet, other, gain, gate, upper, e_gate, e_up, e_down):
    rows, width = packet.shape
    return pl.pallas_call(
        routed_kernel,
        out_shape=(
            jax.ShapeDtypeStruct((rows, width // 2), BF16),
            jax.ShapeDtypeStruct((rows, e_gate.shape[0]), BF16),
        ),
        in_specs=[VMEM] * 8,
        out_specs=(VMEM, VMEM),
        compiler_params=pltpu.CompilerParams(vmem_limit_bytes=24 << 20),
        name="routed",
    )(packet, other, gain, gate, upper, e_gate, e_up, e_down)


def rest_kernel(packet, other, gain, gate, upper, d_gate, d_up, d_down, hidden, e_down, mine, share):
    half = packet.shape[1] // 2
    core = this_core()
    columns = columns_of(1 - core, half)
    at = slice(half, 2 * half)
    rows = scaled(other, at, gain, 1 - core)
    gate = gate[...] + dot_t(rows, d_gate[:, columns])
    upper = upper[...] + dot_t(rows, d_up[:, columns])
    value = gated(gate, upper, row_scale(packet, other, at))
    columns = columns_of(core, half)
    share[...] = dot(value, d_down[:, columns]).astype(BF16)
    mine[...] = dot(hidden[...], e_down[:, columns]).astype(BF16)


def rest(packet, other, gain, gate, upper, d_gate, d_up, d_down, hidden, e_down):
    rows, width = packet.shape
    half = jax.ShapeDtypeStruct((rows, width // 2), BF16)
    return pl.pallas_call(
        rest_kernel,
        out_shape=(half, half),
        in_specs=[VMEM] * 10,
        out_specs=(VMEM, VMEM),
        compiler_params=pltpu.CompilerParams(vmem_limit_bytes=24 << 20),
        name="rest",
    )(packet, other, gain, gate, upper, d_gate, d_up, d_down, hidden, e_down)


def merge_kernel(part, other_part, share, packet):
    half = part.shape[1]
    packet[:, :half] = (part[...].astype(F32) + other_part[...].astype(F32)).astype(BF16)
    packet[:, half:] = share[...]


def merge(part, other_part, share):
    rows, half = part.shape
    return pl.pallas_call(
        merge_kernel,
        out_shape=jax.ShapeDtypeStruct((rows, 2 * half), BF16),
        in_specs=[VMEM] * 3,
        out_specs=VMEM,
        compiler_params=pltpu.CompilerParams(vmem_limit_bytes=8 << 20),
        name="merge",
    )(part, other_part, share)


def combine_kernel(pick, packet, mix, place, out):
    seqs, half = out.shape
    group = 8
    moe = dot(pick[...], packet[:, :half])
    total = moe[:seqs] + moe[seqs:]
    parts = packet[:, half:].astype(F32)
    dense = jnp.sum(parts.reshape(-1, group, half), axis=0)
    dense = sigmoid(by_core(mix[...], this_core())[0]) * dense
    where = place[...]
    for r in range(group):
        total = total + where[:, r : r + 1] * dense[r : r + 1]
    out[...] = total.astype(BF16)


def combine(pick, packet, mix, place):
    width = mix.shape[0]
    return pl.pallas_call(
        combine_kernel,
        out_shape=jax.ShapeDtypeStruct((pick.shape[0] // 2, width // 2), BF16),
        in_specs=[VMEM] * 4,
        out_specs=VMEM,
        compiler_params=pltpu.CompilerParams(vmem_limit_bytes=8 << 20),
        name="combine",
    )(pick, packet, mix.reshape(1, width), place)


def routing(local_routes, experts, capacity):
    flat = local_routes.reshape(-1)
    onehot = (flat[:, None] == jnp.arange(experts, dtype=jnp.int32)[None, :]).astype(jnp.int32)
    before = jnp.cumsum(onehot, axis=0) - onehot
    slot = jnp.sum(before * onehot, axis=1)
    where = (flat * capacity + slot).reshape(local_routes.shape)
    return where[:, :, None] == jnp.arange(experts * capacity, dtype=jnp.int32)[None, None, :]


def core_swap(x):
    return lax.ppermute(x, "tp", [(t, t ^ 1) for t in range(8)])


def added(mine, other):
    return (mine.astype(F32) + other.astype(F32)).astype(BF16)


def from_chips(mine):
    return [lax.ppermute(mine, "tp", [(t, t ^ d) for t in range(8)]) for d in (4, 2, 6)]


def chip_sum(mine, far, near, across):
    return (mine.astype(F32) + near.astype(F32)) + (far.astype(F32) + across.astype(F32))


def tables(routes, route_weights, chip, share_rows, experts, capacity):
    seqs = routes.shape[0]
    hits = routing(routes, experts, capacity)
    slots = jnp.any(hits, axis=1)
    pick = jnp.sum(hits * route_weights[:, :, None], axis=1)
    high = pick.astype(BF16)
    low = (pick - high.astype(F32)).astype(BF16)
    pick = jnp.concatenate([high, low], axis=0)
    token = jnp.arange(seqs, dtype=jnp.int32)[:, None]
    row = jnp.arange(slots.shape[1], dtype=jnp.int32)[None, :]
    place = chip * share_rows + row % share_rows == token
    table = jnp.concatenate([slots, place], axis=1).astype(BF16).T
    return table, pick, place[:, :share_rows].astype(F32)


def local(
    tokens,
    state,
    norm_gain,
    w_query,
    w_forget,
    w_input,
    w_outgate,
    forget_floor,
    head_gain,
    w_out,
    ffn_gain,
    routes,
    route_weights,
    expert_gate,
    expert_up,
    expert_down,
    dense_gate,
    dense_up,
    dense_down,
    dense_mix,
):
    seqs, width = tokens.shape
    tp = lax.axis_index("tp")
    core, chip = tp % 2, tp // 2
    half = width // 2
    groups = lax.axis_size("ep")
    experts = groups * expert_gate.shape[0]
    top = routes.shape[1]
    capacity = 2 * seqs * top // experts
    share_rows = 2 * seqs // lax.axis_size("tp")

    new_state, mine, theirs = mixer(
        tokens, state, norm_gain, w_query, w_forget, w_input, w_outgate, forget_floor, head_gain, w_out
    )
    mine = added(mine, core_swap(theirs))
    mine, routes, route_weights = lax.optimization_barrier((mine, routes, route_weights))
    matrices = tables(routes, route_weights, chip, share_rows, experts, capacity)
    *others, table, pick, place = lax.optimization_barrier((*from_chips(mine), *matrices))
    mixout = chip_sum(mine, *others)
    resid = lax.dynamic_slice_in_dim(tokens, core * half, half, 1).astype(F32) + mixout
    packet = build(table, resid).reshape(groups, capacity, width)
    packet = lax.all_to_all(packet, "ep", split_axis=0, concat_axis=0, tiled=True)
    packet = packet.reshape(groups * capacity, width)
    other = core_swap(packet)
    gain = ffn_gain.reshape(1, width)
    e_gate, e_up, e_down = expert_gate[0].T, expert_up[0].T, expert_down[0]
    d_gate, d_up = dense_gate.T, dense_up.T
    gate_e, up_e, gate_d, up_d = front(
        packet, gain, e_gate, e_up, d_gate, d_up, e_down, dense_down
    )
    theirs, hidden = routed(packet, other, gain, gate_e, up_e, e_gate, e_up, e_down)
    part, share = rest(
        packet, other, gain, gate_d, up_d, d_gate, d_up, dense_down, hidden, e_down
    )
    packet = merge(part, core_swap(theirs), share).reshape(groups, capacity, width)
    packet = lax.all_to_all(packet, "ep", split_axis=0, concat_axis=0, tiled=True)
    mine = combine(pick, packet.reshape(groups * capacity, width), dense_mix, place)
    mixed = (resid + chip_sum(mine, *from_chips(mine))).astype(BF16)
    other = core_swap(mixed)
    first = jnp.where(core == 0, mixed, other)
    second = jnp.where(core == 0, other, mixed)
    return (jnp.concatenate([first, second], axis=1), new_state)


def solution(mesh):
    in_specs = (
        P("ep", None),
        P("ep", "tp", None, None),
        P(),
        P(None, "tp"),
        P(None, "tp"),
        P(None, "tp"),
        P(None, "tp"),
        P("tp"),
        P(),
        P("tp", None),
        P(),
        P("ep", None),
        P("ep", None),
        P("ep", None, "tp"),
        P("ep", None, "tp"),
        P("ep", "tp", None),
        P(None, "ep"),
        P(None, "ep"),
        P("ep", None),
        P(),
    )
    out_specs = (P("ep", None), P("ep", "tp", None, None))
    return jax.shard_map(local, mesh=mesh, in_specs=in_specs, out_specs=out_specs, check_vma=False)
```

```python
import jax
import jax.numpy as jnp
from jax import lax
from jax.experimental import pallas as pl
from jax.experimental.pallas import tpu as pltpu
from jax.sharding import PartitionSpec as P


EPS = 1e-06
F32 = jnp.float32
BF16 = jnp.bfloat16
HBM = pl.BlockSpec(memory_space=pltpu.HBM)
VMEM = pl.BlockSpec(memory_space=pltpu.VMEM)


CHUNKS = 4


def dot(a, b):
    return jnp.dot(a, b, preferred_element_type=F32)


def dot_t(a, b):
    return lax.dot_general(a, b, (((1,), (1,)), ((), ())), preferred_element_type=F32)


def mean_scale(x):
    return lax.rsqrt(jnp.mean(x * x, axis=-1, keepdims=True) + EPS)


def this_core():
    return lax.rem(lax.axis_index("tp"), 2)


def by_core(x, core):
    half = x.shape[1] // 2
    low, high = x[:, :half], x[:, half:]
    return jnp.where(core == 0, low, high), jnp.where(core == 0, high, low)


def sigmoid(x):
    return 1.0 / (1.0 + jnp.exp(-x))


def mixer_kernel(
    tokens_in,
    gain_in,
    floor_in,
    head_gain_in,
    state,
    w_query,
    w_forget,
    w_input,
    w_outgate,
    w_out,
    new_state,
    mine,
    theirs,
    tokens,
    gain,
    floor,
    head_gain,
    w_buf,
    wo_buf,
    held,
    spread,
    columns,
    values,
    read,
    small_sem,
    w_sem,
    wo_sem,
    in_sem,
    out_sem,
):
    seqs = tokens.shape[0]
    heads, size = held.shape[1:3]
    step = seqs // CHUNKS
    core = this_core()
    small = [
        pltpu.make_async_copy(a, b, small_sem.at[i])
        for i, (a, b) in enumerate(
            ((tokens_in, tokens), (gain_in, gain), (floor_in, floor), (head_gain_in, head_gain))
        )
    ]
    for load in small:
        load.start()
    loads = [
        pltpu.make_async_copy(w, w_buf.at[i], w_sem.at[i])
        for i, w in enumerate((w_forget, w_query, w_input, w_outgate))
    ]
    for load in loads[:3]:
        load.start()

    def fetch(j):
        rows = pl.ds(j * step, step)
        return pltpu.make_async_copy(state.at[rows], held.at[rows], in_sem.at[j])

    def flush_half(j, part):
        rows = pl.ds(j * step + part * (step // 2), step // 2)
        return pltpu.make_async_copy(held.at[rows], new_state.at[rows], out_sem.at[2 * j + part])

    for load in small[:2]:
        load.wait()
    x = tokens[...].astype(F32)
    normed = (x * mean_scale(x) * gain[...]).astype(BF16)
    for j in range(2):
        fetch(j).start()
    for load in small[2:]:
        load.wait()
    base = floor[...]
    row = lax.broadcasted_iota(jnp.int32, spread.shape[1:], 0)
    lane = lax.broadcasted_iota(jnp.int32, spread.shape[1:], 1)
    source = jnp.where(row < 3 * seqs, row % seqs - lane // size, -1)
    for p in range(spread.shape[0]):
        spread[p] = jnp.where(source == 2 * p, 1.0, 0.0).astype(BF16)
    loads[0].wait()
    for j in range(2, CHUNKS):
        fetch(j).start()
    keep = base + (1.0 - base) * sigmoid(dot(normed, w_buf[0]))
    loads[1].wait()
    loads[3].start()
    load_out = pltpu.make_async_copy(w_out, wo_buf, wo_sem)
    load_out.start()
    zq = dot(normed, w_buf[1])
    both = jnp.concatenate([keep, zq * sigmoid(zq)], axis=1)
    parts = []
    for _ in range(3):
        parts.append(both.astype(BF16).astype(F32))
        both = both - parts[-1]
    parts.append(jnp.zeros((size - 3 * seqs, both.shape[1]), F32))
    columns[...] = jnp.concatenate(parts, axis=0).T.astype(BF16)
    loads[2].wait()
    values[...] = dot(normed, w_buf[2])

    def body(j, carry):
        fetch(j).wait()
        rows = pl.ds(pl.multiple_of(j * step, step), step)
        block = values[rows, :]
        reads = [[None] * heads for _ in range(step)]
        for p in range(step // 2):
            one = spread[j * (step // 2) + p]
            for h in range(heads):
                at = h * size
                keeps = dot(columns[at : at + size, :], one)
                queries = dot(columns[(heads + h) * size : (heads + h + 1) * size, :], one)
                for i in range(2):
                    t = 2 * p + i
                    v = block[t : t + 1, at : at + size]
                    lanes = slice(i * size, (i + 1) * size)
                    new = v + keeps[:, lanes] * (held[j * step + t, h] - v)
                    held[j * step + t, h] = new
                    reads[t][h] = jnp.sum(queries[:, lanes] * new, axis=0, keepdims=True)
            if p % (step // 4) == step // 4 - 1:
                flush_half(j, p // (step // 4)).start()
        read[rows, :] = jnp.concatenate([jnp.concatenate(r, axis=1) for r in reads], axis=0)
        return carry

    lax.fori_loop(0, CHUNKS, body, 0)
    loads[3].wait()
    zg = dot(normed, w_buf[3])
    gate = zg * sigmoid(zg)
    outs = []
    for h in range(heads):
        lanes = slice(h * size, (h + 1) * size)
        r = read[:, lanes]
        outs.append(r * mean_scale(r) * head_gain[...] * gate[:, lanes])
    headout = jnp.concatenate(outs, axis=1).astype(BF16)
    load_out.wait()
    block = dot(headout, wo_buf[...])
    mine[...], theirs[...] = by_core(block.astype(BF16), core)
    for j in range(CHUNKS):
        for part in range(2):
            flush_half(j, part).wait()


def mixer(tokens, state, norm_gain, w_query, w_forget, w_input, w_outgate, floor, head_gain, w_out):
    seqs, width = tokens.shape
    channels = w_query.shape[1]
    half = jax.ShapeDtypeStruct((seqs, width // 2), BF16)
    size = state.shape[3]
    return pl.pallas_call(
        mixer_kernel,
        out_shape=(jax.ShapeDtypeStruct(state.shape, state.dtype), half, half),
        in_specs=[HBM] * 10,
        out_specs=(HBM, VMEM, VMEM),
        scratch_shapes=[
            pltpu.VMEM((seqs, width), BF16),
            pltpu.VMEM((1, width), F32),
            pltpu.VMEM((1, channels), F32),
            pltpu.VMEM((1, state.shape[3]), F32),
            pltpu.VMEM((4, width, channels), BF16),
            pltpu.VMEM((channels, width), BF16),
            pltpu.VMEM(state.shape, F32),
            pltpu.VMEM((seqs // 2, size, 2 * size), BF16),
            pltpu.VMEM((2 * channels, size), BF16),
            pltpu.VMEM((seqs, channels), F32),
            pltpu.VMEM((seqs, channels), F32),
            pltpu.SemaphoreType.DMA((4,)),
            pltpu.SemaphoreType.DMA((4,)),
            pltpu.SemaphoreType.DMA,
            pltpu.SemaphoreType.DMA((CHUNKS,)),
            pltpu.SemaphoreType.DMA((2 * CHUNKS,)),
        ],
        compiler_params=pltpu.CompilerParams(vmem_limit_bytes=20 << 20),
        name="mixer",
    )(
        *(
            pltpu.with_memory_space_constraint(x, pltpu.HBM)
            for x in (
                tokens,
                norm_gain.reshape(1, width),
                floor.reshape(1, channels),
                head_gain.reshape(1, -1),
                state,
                w_query,
                w_forget,
                w_input,
                w_outgate,
                w_out,
            )
        )
    )


def build_kernel(table, resid, packet):
    half = resid.shape[1]
    rows = dot(table[...], resid[...].astype(BF16)).astype(BF16)
    packet[:, :half] = rows[: packet.shape[0]]
    packet[:, half:] = rows[packet.shape[0] :]


def build(table, resid):
    rows, half = table.shape[0] // 2, resid.shape[1]
    return pl.pallas_call(
        build_kernel,
        out_shape=jax.ShapeDtypeStruct((rows, 2 * half), BF16),
        in_specs=[VMEM] * 2,
        out_specs=VMEM,
        compiler_params=pltpu.CompilerParams(vmem_limit_bytes=8 << 20),
        cost_estimate=pl.CostEstimate(flops=10**10, bytes_accessed=10**8, transcendentals=0),
        name="build",
    )(table, resid)


def columns_of(core, half):
    return pl.ds(pl.multiple_of(core * half, half), half)


def scaled(packet, at, gain, core):
    half = packet.shape[1] // 2
    factor = jnp.where(core == 0, gain[:, :half], gain[:, half:])
    return (packet[:, at].astype(F32) * factor).astype(BF16)


def row_scale(packet, other, at):
    mine, theirs = packet[:, at].astype(F32), other[:, at].astype(F32)
    total = jnp.sum(mine * mine, axis=-1, keepdims=True)
    total = total + jnp.sum(theirs * theirs, axis=-1, keepdims=True)
    return lax.rsqrt(total / packet.shape[1] + EPS)


def gated(gate, upper, scale):
    gate = gate * scale
    return (gate * sigmoid(gate) * (upper * scale)).astype(BF16)


def front_kernel(packet, gain, e_gate, e_up, d_gate, d_up, e_down, d_down, *outs):
    half = packet.shape[1] // 2
    core = this_core()
    columns = columns_of(core, half)
    routed = scaled(packet, slice(0, half), gain, core)
    share = scaled(packet, slice(half, 2 * half), gain, core)
    outs[0][...] = dot_t(routed, e_gate[:, columns])
    outs[1][...] = dot_t(routed, e_up[:, columns])
    outs[2][...] = dot_t(share, d_gate[:, columns])
    outs[3][...] = dot_t(share, d_up[:, columns])


def front(packet, gain, *weights):
    rows, _ = packet.shape
    return pl.pallas_call(
        front_kernel,
        out_shape=[jax.ShapeDtypeStruct((rows, w.shape[0]), F32) for w in weights[:4]],
        in_specs=[VMEM] * 8,
        out_specs=[VMEM] * 4,
        compiler_params=pltpu.CompilerParams(vmem_limit_bytes=28 << 20),
        name="front",
    )(packet, gain, *weights)


def routed_kernel(packet, other, gain, gate, upper, e_gate, e_up, e_down, theirs, hidden):
    half = packet.shape[1] // 2
    there = 1 - this_core()
    columns = columns_of(there, half)
    at = slice(0, half)
    rows = scaled(other, at, gain, there)
    gate = gate[...] + dot_t(rows, e_gate[:, columns])
    upper = upper[...] + dot_t(rows, e_up[:, columns])
    value = gated(gate, upper, row_scale(packet, other, at))
    hidden[...] = value
    theirs[...] = dot(value, e_down[:, columns]).astype(BF16)


def routed(packet, other, gain, gate, upper, e_gate, e_up, e_down):
    rows, width = packet.shape
    return pl.pallas_call(
        routed_kernel,
        out_shape=(
            jax.ShapeDtypeStruct((rows, width // 2), BF16),
            jax.ShapeDtypeStruct((rows, e_gate.shape[0]), BF16),
        ),
        in_specs=[VMEM] * 8,
        out_specs=(VMEM, VMEM),
        compiler_params=pltpu.CompilerParams(vmem_limit_bytes=24 << 20),
        name="routed",
    )(packet, other, gain, gate, upper, e_gate, e_up, e_down)


def rest_kernel(packet, other, gain, gate, upper, d_gate, d_up, d_down, hidden, e_down, mine, share):
    half = packet.shape[1] // 2
    core = this_core()
    columns = columns_of(1 - core, half)
    at = slice(half, 2 * half)
    rows = scaled(other, at, gain, 1 - core)
    gate = gate[...] + dot_t(rows, d_gate[:, columns])
    upper = upper[...] + dot_t(rows, d_up[:, columns])
    value = gated(gate, upper, row_scale(packet, other, at))
    columns = columns_of(core, half)
    share[...] = dot(value, d_down[:, columns]).astype(BF16)
    mine[...] = dot(hidden[...], e_down[:, columns]).astype(BF16)


def rest(packet, other, gain, gate, upper, d_gate, d_up, d_down, hidden, e_down):
    rows, width = packet.shape
    half = jax.ShapeDtypeStruct((rows, width // 2), BF16)
    return pl.pallas_call(
        rest_kernel,
        out_shape=(half, half),
        in_specs=[VMEM] * 10,
        out_specs=(VMEM, VMEM),
        compiler_params=pltpu.CompilerParams(vmem_limit_bytes=24 << 20),
        name="rest",
    )(packet, other, gain, gate, upper, d_gate, d_up, d_down, hidden, e_down)


def merge_kernel(part, other_part, share, packet):
    half = part.shape[1]
    packet[:, :half] = (part[...].astype(F32) + other_part[...].astype(F32)).astype(BF16)
    packet[:, half:] = share[...]


def merge(part, other_part, share):
    rows, half = part.shape
    return pl.pallas_call(
        merge_kernel,
        out_shape=jax.ShapeDtypeStruct((rows, 2 * half), BF16),
        in_specs=[VMEM] * 3,
        out_specs=VMEM,
        compiler_params=pltpu.CompilerParams(vmem_limit_bytes=8 << 20),
        name="merge",
    )(part, other_part, share)


def combine_kernel(pick, packet, mix, place, out):
    seqs, half = out.shape
    group = 8
    moe = dot(pick[...], packet[:, :half])
    total = moe[:seqs] + moe[seqs:]
    parts = packet[:, half:].astype(F32)
    dense = jnp.sum(parts.reshape(-1, group, half), axis=0)
    dense = sigmoid(by_core(mix[...], this_core())[0]) * dense
    where = place[...]
    for r in range(group):
        total = total + where[:, r : r + 1] * dense[r : r + 1]
    out[...] = total.astype(BF16)


def combine(pick, packet, mix, place):
    width = mix.shape[0]
    return pl.pallas_call(
        combine_kernel,
        out_shape=jax.ShapeDtypeStruct((pick.shape[0] // 2, width // 2), BF16),
        in_specs=[VMEM] * 4,
        out_specs=VMEM,
        compiler_params=pltpu.CompilerParams(vmem_limit_bytes=8 << 20),
        name="combine",
    )(pick, packet, mix.reshape(1, width), place)


def routing(local_routes, experts, capacity):
    flat = local_routes.reshape(-1)
    onehot = (flat[:, None] == jnp.arange(experts, dtype=jnp.int32)[None, :]).astype(jnp.int32)
    before = jnp.cumsum(onehot, axis=0) - onehot
    slot = jnp.sum(before * onehot, axis=1)
    where = (flat * capacity + slot).reshape(local_routes.shape)
    return where[:, :, None] == jnp.arange(experts * capacity, dtype=jnp.int32)[None, None, :]


def core_swap(x):
    return lax.ppermute(x, "tp", [(t, t ^ 1) for t in range(8)])


def added(mine, other):
    return (mine.astype(F32) + other.astype(F32)).astype(BF16)


def from_chips(mine):
    others = []
    for d in (4, 2, 6):
        others.append(lax.ppermute(mine, "tp", [(t, t ^ d) for t in range(8)]))
    return others


def chip_sum(mine, far, near, across):
    return (mine.astype(F32) + near.astype(F32)) + (far.astype(F32) + across.astype(F32))


def tables(routes, route_weights, chip, share_rows, experts, capacity):
    seqs = routes.shape[0]
    hits = routing(routes, experts, capacity)
    slots = jnp.any(hits, axis=1)
    pick = jnp.sum(hits * route_weights[:, :, None], axis=1)
    high = pick.astype(BF16)
    low = (pick - high.astype(F32)).astype(BF16)
    pick = jnp.concatenate([high, low], axis=0)
    token = jnp.arange(seqs, dtype=jnp.int32)[:, None]
    row = jnp.arange(slots.shape[1], dtype=jnp.int32)[None, :]
    place = chip * share_rows + row % share_rows == token
    table = jnp.concatenate([slots, place], axis=1).astype(BF16).T
    return table, pick, place[:, :share_rows].astype(F32)


def local(
    tokens,
    state,
    norm_gain,
    w_query,
    w_forget,
    w_input,
    w_outgate,
    forget_floor,
    head_gain,
    w_out,
    ffn_gain,
    routes,
    route_weights,
    expert_gate,
    expert_up,
    expert_down,
    dense_gate,
    dense_up,
    dense_down,
    dense_mix,
):
    seqs, width = tokens.shape
    tp = lax.axis_index("tp")
    core, chip = tp % 2, tp // 2
    half = width // 2
    groups = lax.axis_size("ep")
    experts = groups * expert_gate.shape[0]
    top = routes.shape[1]
    capacity = 2 * seqs * top // experts
    share_rows = 2 * seqs // lax.axis_size("tp")

    new_state, mine, theirs = mixer(
        tokens, state, norm_gain, w_query, w_forget, w_input, w_outgate, forget_floor, head_gain, w_out
    )
    mine = added(mine, core_swap(theirs))
    mine, routes, route_weights = lax.optimization_barrier((mine, routes, route_weights))
    matrices = tables(routes, route_weights, chip, share_rows, experts, capacity)
    *others, table, pick, place = lax.optimization_barrier((*from_chips(mine), *matrices))
    mixout = chip_sum(mine, *others)
    resid = lax.dynamic_slice_in_dim(tokens, core * half, half, 1).astype(F32) + mixout
    packet = build(table, resid).reshape(groups, capacity, width)
    packet = lax.all_to_all(packet, "ep", split_axis=0, concat_axis=0, tiled=True)
    packet = packet.reshape(groups * capacity, width)
    other = core_swap(packet)
    gain = ffn_gain.reshape(1, width)
    e_gate, e_up, e_down = expert_gate[0].T, expert_up[0].T, expert_down[0]
    d_gate, d_up = dense_gate.T, dense_up.T
    gate_e, up_e, gate_d, up_d = front(
        packet, gain, e_gate, e_up, d_gate, d_up, e_down, dense_down
    )
    theirs, hidden = routed(packet, other, gain, gate_e, up_e, e_gate, e_up, e_down)
    part, share = rest(
        packet, other, gain, gate_d, up_d, d_gate, d_up, dense_down, hidden, e_down
    )
    packet = merge(part, core_swap(theirs), share).reshape(groups, capacity, width)
    packet = lax.all_to_all(packet, "ep", split_axis=0, concat_axis=0, tiled=True)
    mine = combine(pick, packet.reshape(groups * capacity, width), dense_mix, place)
    mixed = (resid + chip_sum(mine, *from_chips(mine))).astype(BF16)
    other = core_swap(mixed)
    first = jnp.where(core == 0, mixed, other)
    second = jnp.where(core == 0, other, mixed)
    return (jnp.concatenate([first, second], axis=1), new_state)


def solution(mesh):
    in_specs = (
        P("ep", None),
        P("ep", "tp", None, None),
        P(),
        P(None, "tp"),
        P(None, "tp"),
        P(None, "tp"),
        P(None, "tp"),
        P("tp"),
        P(),
        P("tp", None),
        P(),
        P("ep", None),
        P("ep", None),
        P("ep", None, "tp"),
        P("ep", None, "tp"),
        P("ep", "tp", None),
        P(None, "ep"),
        P(None, "ep"),
        P("ep", None),
        P(),
    )
    out_specs = (P("ep", None), P("ep", "tp", None, None))


    return jax.shard_map(local, mesh=mesh, in_specs=in_specs, out_specs=out_specs, check_vma=False)
```
